32 devices in a mesh: kv: 16 (over z, y, x), tp: 2 (over core).
Axes of the slice: x: 2, y: 2, z: 4, core: 2. Of those that a mesh axis runs over, the one named last changes fastest.
Arguments:
- residual_in: bfloat16 [96, 2048], P('kv', 'tp'), may hold values from -36 to 36
- gain_pre: float32 [2048], P('tp'), may hold values from 0.1 to 1.9
- gate_pre: bfloat16 [2048, 5632], P('tp', 'kv'), may hold values from -0.125 to 0.125
- up_pre: bfloat16 [2048, 5632], P('tp', 'kv'), may hold values from -0.125 to 0.125
- down_pre: bfloat16 [5632, 2048], P('kv', 'tp'), may hold values from -0.078125 to 0.078125
- gain_mix: float32 [2048], replicated, may hold values from 0.1 to 1.9
- query_weight: bfloat16 [2048, 2048], P('kv', 'tp'), may hold values from -0.125 to 0.125
- forget_weight: bfloat16 [2048, 2048], P('kv', 'tp'), may hold values from -0.125 to 0.125
- value_weight: bfloat16 [2048, 2048], P('kv', 'tp'), may hold values from -0.125 to 0.125
- outgate_weight: bfloat16 [2048, 2048], P('kv', 'tp'), may hold values from -0.125 to 0.125
- lower_bound: float32 [2048], P('tp'), may hold values from 0.05 to 0.95
- head_gain: float32 [2048], P('tp'), may hold values from 0.1 to 1.9
- out_weight: bfloat16 [2048, 2048], P('tp'), may hold values from -0.125 to 0.125
- gain_post: float32 [2048], P('tp'), may hold values from 0.1 to 1.9
- gate_post: bfloat16 [2048, 5632], P('tp', 'kv'), may hold values from -0.125 to 0.125
- up_post: bfloat16 [2048, 5632], P('tp', 'kv'), may hold values from -0.125 to 0.125
- down_post: bfloat16 [5632, 2048], P('kv', 'tp'), may hold values from -0.078125 to 0.078125
- memory_state: float32 [96, 16, 128, 128], P('kv', 'tp'), may hold values from -4 to 4
Outputs:
- layer_out: bfloat16 [96, 2048], P('kv', 'tp')
- next_state: float32 [96, 16, 128, 128], P('kv', 'tp')
The draws below stay inside these ranges and needn't reach their ends.
All inputs are finite; a program needn't handle non-finite values.
Results may differ from the reference program's by a relative error of at most 0.014.
Values may be sent and summed in bfloat16 or wider, within the bound.
A program may use at most 64 MiB of HBM per device.

```python
import math
import jax
import jax.numpy as jnp
from jax import lax

D = 2048
FF = 5632
HEADS = 16
HEAD_DIM = 128
HW = 2048
BATCH = 96


def draw_residual_in(key, part):
    key_base = jax.random.fold_in(key, 11)
    key_cols = jax.random.fold_in(key, 12)
    key_rows = jax.random.fold_in(key, 13)
    column_pos = jnp.arange(D, dtype=jnp.float32) / D
    col_scale = 4.0 ** column_pos * jax.random.uniform(key_cols, (D,), jnp.float32, 0.5, 1.5)
    row_scale = jnp.exp(jax.random.uniform(key_rows, (BATCH, 1), jnp.float32, 0.0, math.log(10.0)))
    base_vals = jnp.clip(jax.random.normal(key_base, (BATCH, D), jnp.float32), -4.0, 4.0)
    return (0.15 * base_vals * col_scale[None, :] * row_scale).astype(jnp.bfloat16)


def block_scale(key, dims, split, smallest, high):
    factor_of = 1.0
    for dim, shards_of in split:
        heights = jax.random.uniform(jax.random.fold_in(jax.random.fold_in(key, 6), dim), (shards_of,), jnp.float32, smallest / len(split), high / len(split))
        factor_of = factor_of * jnp.repeat(jnp.exp(heights), dims[dim] // shards_of).reshape((-1,) + (1,) * (len(dims) - 1 - dim))
    return factor_of


def bell_draw(rng, extent, scale, reach, cuts=(), kind=jnp.bfloat16):
    array = scale * jax.random.normal(rng, extent, jnp.float32)
    if cuts:
        array = array * block_scale(rng, extent, cuts, -0.22, 0.18)
    return jnp.clip(array, -reach, reach).astype(kind)


def setup_inputs(seed: int = 0) -> dict:
    key_of = jax.random.split(jax.random.key(seed), 19)
    residual_in = draw_residual_in(jax.random.fold_in(key_of[18], 71), 0)
    gain_pre = jnp.clip(1.0 + 0.18 * jax.random.normal(key_of[1], (D,), jnp.float32), 0.1, 1.9)
    gate_pre = bell_draw(key_of[2], (D, FF), D ** -0.5, 0.125, ((0, 2), (1, 16)))
    up_pre = bell_draw(key_of[3], (D, FF), D ** -0.5, 0.125, ((0, 2), (1, 16)))
    down_pre = bell_draw(key_of[4], (FF, D), FF ** -0.5, 0.078125, ((0, 16), (1, 2)))
    gain_mix = jnp.clip(1.0 + 0.18 * jax.random.normal(key_of[5], (D,), jnp.float32), 0.1, 1.9)
    query_weight = bell_draw(key_of[6], (D, HW), D ** -0.5, 0.125, ((0, 16), (1, 2)))
    forget_weight = bell_draw(key_of[7], (D, HW), D ** -0.5, 0.125, ((0, 16), (1, 2)))
    value_weight = bell_draw(key_of[8], (D, HW), D ** -0.5, 0.125, ((0, 16), (1, 2)))
    outgate_weight = bell_draw(key_of[9], (D, HW), D ** -0.5, 0.125, ((0, 16), (1, 2)))
    lower_bound = jnp.clip(0.05 + 0.9 * jax.random.uniform(key_of[10], (HW,), jnp.float32) ** block_scale(key_of[10], (HW,), ((0, 2),), -0.2, 0.2), 0.05, 0.95)
    head_gain = jnp.clip(1.0 + 0.18 * jax.random.normal(key_of[11], (HW,), jnp.float32), 0.1, 1.9)
    out_weight = bell_draw(key_of[12], (HW, D), HW ** -0.5, 0.125, ((0, 2),))
    gain_post = jnp.clip(1.0 + 0.18 * jax.random.normal(key_of[13], (D,), jnp.float32), 0.1, 1.9)
    gate_post = bell_draw(key_of[14], (D, FF), D ** -0.5, 0.125, ((0, 2), (1, 16)))
    up_post = bell_draw(key_of[15], (D, FF), D ** -0.5, 0.125, ((0, 2), (1, 16)))
    down_post = bell_draw(key_of[16], (FF, D), FF ** -0.5, 0.078125, ((0, 16), (1, 2)))
    memory_state = bell_draw(key_of[17], (BATCH, HEADS, HEAD_DIM, HEAD_DIM), 0.5, 4.0, ((0, 16), (1, 2)), jnp.float32)
    return dict(residual_in=residual_in, gain_pre=gain_pre, gate_pre=gate_pre, up_pre=up_pre, down_pre=down_pre, gain_mix=gain_mix, query_weight=query_weight, forget_weight=forget_weight, value_weight=value_weight, outgate_weight=outgate_weight, lower_bound=lower_bound, head_gain=head_gain, out_weight=out_weight, gain_post=gain_post, gate_post=gate_post, up_post=up_post, down_post=down_post, memory_state=memory_state)


EPSILON = 1e-06

def channel_mixer(stream, gain_vec, gate_weight, up_weight, down_weight):
    widened = stream.astype(jnp.float32)
    inverse = lax.rsqrt(lax.optimization_barrier(jnp.mean(widened * widened, axis=1, keepdims=True)) + EPSILON)
    scaled = (widened * gain_vec).astype(jnp.bfloat16)
    gate_sum = jnp.dot(scaled, gate_weight, preferred_element_type=jnp.float32) * inverse
    up_sum = jnp.dot(scaled, up_weight, preferred_element_type=jnp.float32) * inverse
    hidden = (jax.nn.silu(gate_sum) * up_sum).astype(jnp.bfloat16)
    return jnp.dot(hidden, down_weight, preferred_element_type=jnp.float32)

def token_mixer(stream, gain_mix, query_weight, forget_weight, value_weight, outgate_weight, lower_bound, head_gain, out_weight, memory_state):
    widened = stream.astype(jnp.float32)
    inverse = lax.rsqrt(lax.optimization_barrier(jnp.mean(widened * widened, axis=1, keepdims=True)) + EPSILON)
    scaled = (widened * gain_mix).astype(jnp.bfloat16)
    batch_rows = stream.shape[0]

    def project(weight_mat):
        product = jnp.dot(scaled, weight_mat, preferred_element_type=jnp.float32) * inverse
        return product.reshape(batch_rows, HEADS, HEAD_DIM)
    query_pre = project(query_weight)
    forget_pre = project(forget_weight)
    value_pre = project(value_weight)
    outgate_pre = project(outgate_weight)
    floor_rate = lower_bound.reshape(HEADS, HEAD_DIM)
    log_keep = jnp.logaddexp(jnp.log(floor_rate), jnp.log1p(-floor_rate) + jax.nn.log_sigmoid(forget_pre))
    inject = (1.0 - floor_rate) * jax.nn.sigmoid(-forget_pre)
    next_state = jnp.exp(log_keep)[..., None] * memory_state + inject[..., None] * value_pre[:, :, None, :]
    readout = jnp.einsum('bhk,bhkv->bhv', jax.nn.silu(query_pre), next_state, precision=lax.Precision.HIGHEST)
    normed = readout * lax.rsqrt(lax.optimization_barrier(jnp.mean(readout * readout, axis=2, keepdims=True)) + EPSILON) * head_gain.reshape(HEADS, HEAD_DIM)
    mixed_heads = (normed * jax.nn.silu(outgate_pre)).reshape(batch_rows, HEADS * HEAD_DIM).astype(jnp.bfloat16)
    mixed = jnp.dot(mixed_heads, out_weight, preferred_element_type=jnp.float32)
    return (mixed, next_state)

def reference(residual_in, gain_pre, gate_pre, up_pre, down_pre, gain_mix, query_weight, forget_weight, value_weight, outgate_weight, lower_bound, head_gain, out_weight, gain_post, gate_post, up_post, down_post, memory_state):
    branch_a = channel_mixer(residual_in, gain_pre, gate_pre, up_pre, down_pre)
    stream_a = (residual_in.astype(jnp.float32) + 0.5 * branch_a).astype(jnp.bfloat16)
    mixed, next_state = token_mixer(stream_a, gain_mix, query_weight, forget_weight, value_weight, outgate_weight, lower_bound, head_gain, out_weight, memory_state)
    stream_b = (stream_a.astype(jnp.float32) + mixed).astype(jnp.bfloat16)
    branch_b = channel_mixer(stream_b, gain_post, gate_post, up_post, down_post)
    layer_out = (stream_b.astype(jnp.float32) + 0.5 * branch_b).astype(jnp.bfloat16)
    return (layer_out, next_state)
```

```python
import functools

import jax
import jax.numpy as jnp
from jax import lax
from jax.experimental import pallas as pl
from jax.experimental.pallas import tpu as pltpu
from jax.sharding import PartitionSpec as P

D = 2048
HEAD_DIM = 128


EPSILON = 1e-06


def channel_mixer(row_block, gain_vec, gate_weight, up_weight, down_weight):
    gathered = lax.all_gather(row_block, "kv", axis=0, tiled=True)
    widened = gathered.astype(jnp.float32)
    part_squares = jnp.sum(widened * widened, axis=1)
    scaled = (widened * gain_vec).astype(jnp.bfloat16)
    gate_part = jnp.dot(scaled, gate_weight, preferred_element_type=jnp.float32)
    up_part = jnp.dot(scaled, up_weight, preferred_element_type=jnp.float32)
    gate_share, up_share, square_share = (
        lax.psum_scatter(
            gate_part.astype(jnp.bfloat16), "tp", scatter_dimension=0, tiled=True
        ).astype(jnp.float32),
        lax.psum_scatter(
            up_part.astype(jnp.bfloat16), "tp", scatter_dimension=0, tiled=True
        ).astype(jnp.float32),
        lax.psum_scatter(
            part_squares.astype(jnp.bfloat16), "tp", scatter_dimension=0, tiled=True
        ).astype(jnp.float32),
    )
    share_inverse = lax.rsqrt(square_share / D + EPSILON)[:, None]
    hidden_share = (jax.nn.silu(gate_share * share_inverse) * (up_share * share_inverse)).astype(
        jnp.bfloat16
    )
    hidden = lax.all_gather(hidden_share, "tp", axis=0, tiled=True)
    return lax.psum_scatter(
        jnp.dot(hidden, down_weight, preferred_element_type=jnp.float32),
        "kv",
        scatter_dimension=0,
        tiled=True,
    )


def token_mixer(
    stream_a,
    gain_mix,
    query_weight,
    forget_weight,
    value_weight,
    outgate_weight,
    lower_bound,
    head_gain,
    out_weight,
    memory_state,
):
    full_rows = lax.all_gather(stream_a, "tp", axis=1, tiled=True)
    widened = full_rows.astype(jnp.float32)
    inverse = lax.rsqrt(jnp.mean(widened * widened, axis=1, keepdims=True) + EPSILON)
    scaled = (widened * gain_mix).astype(jnp.bfloat16)
    weights = (query_weight, forget_weight, value_weight, outgate_weight)
    blocks = lax.all_to_all(scaled, "kv", split_axis=1, concat_axis=0, tiled=True)
    joined = jnp.concatenate(weights, axis=1)
    projected = lax.psum_scatter(
        jnp.dot(blocks, joined, preferred_element_type=jnp.float32),
        "kv",
        scatter_dimension=0,
        tiled=True,
    )
    projected = projected * inverse
    seq_rows = scaled.shape[0]
    local_heads = query_weight.shape[1] // HEAD_DIM
    reshaped = projected.reshape(seq_rows, 4, local_heads, HEAD_DIM)
    query_pre = reshaped[:, 0]
    forget_pre = reshaped[:, 1]
    value_pre = reshaped[:, 2]
    outgate_pre = reshaped[:, 3]
    floor_rate = lower_bound.reshape(local_heads, HEAD_DIM)
    log_keep = jnp.logaddexp(
        jnp.log(floor_rate), jnp.log1p(-floor_rate) + jax.nn.log_sigmoid(forget_pre)
    )
    inject = (1.0 - floor_rate) * jax.nn.sigmoid(-forget_pre)
    next_state = (
        jnp.exp(log_keep)[..., None] * memory_state + inject[..., None] * value_pre[:, :, None, :]
    )
    readout = jnp.einsum(
        "bhk,bhkv->bhv", jax.nn.silu(query_pre), next_state, precision=lax.Precision.HIGHEST
    )
    normed = (
        readout
        * lax.rsqrt(jnp.mean(readout * readout, axis=2, keepdims=True) + EPSILON)
        * head_gain.reshape(local_heads, HEAD_DIM)
    )
    mixed_heads = (
        (normed * jax.nn.silu(outgate_pre))
        .reshape(seq_rows, local_heads * HEAD_DIM)
        .astype(jnp.bfloat16)
    )
    partial_out = jnp.dot(mixed_heads, out_weight, preferred_element_type=jnp.float32)
    mixed = lax.psum_scatter(
        partial_out.astype(jnp.bfloat16), "tp", scatter_dimension=1, tiled=True
    ).astype(jnp.float32)
    return (mixed, next_state)


def shards(
    residual_in,
    gain_pre,
    gate_pre,
    up_pre,
    down_pre,
    gain_mix,
    query_weight,
    forget_weight,
    value_weight,
    outgate_weight,
    lower_bound,
    head_gain,
    out_weight,
    gain_post,
    gate_post,
    up_post,
    down_post,
    memory_state,
):
    branch_a = channel_mixer(residual_in, gain_pre, gate_pre, up_pre, down_pre)
    stream_a = (residual_in.astype(jnp.float32) + 0.5 * branch_a).astype(jnp.bfloat16)
    mixed, next_state = token_mixer(
        stream_a,
        gain_mix,
        query_weight,
        forget_weight,
        value_weight,
        outgate_weight,
        lower_bound,
        head_gain,
        out_weight,
        memory_state,
    )
    stream_b = (stream_a.astype(jnp.float32) + mixed).astype(jnp.bfloat16)
    branch_b = channel_mixer(stream_b, gain_post, gate_post, up_post, down_post)
    layer_out = (stream_b.astype(jnp.float32) + 0.5 * branch_b).astype(jnp.bfloat16)
    return (layer_out, next_state)


LANES = 128
GROUPS = 8
PLANE = 4
GATHER_A, WEIGHTS, SCATTER_A, SHARE, ROWS, PROJECT, GATHER_B, SCATTER_B = range(8)
EXCHANGES = 8
FLIPS = (3, 1, 2, 0)


def dot_columns(rows, weight_columns):
    return lax.dot_general(
        rows, weight_columns, (((1,), (1,)), ((), ())), preferred_element_type=jnp.float32
    )


def lanes(group):
    return slice(group * LANES, (group + 1) * LANES)


def fused_layer(
    n_kv,
    residual_ref,
    gain_pre_ref,
    gain_mix_ref,
    lower_ref,
    head_gain_ref,
    gain_post_ref,
    gate_pre_hbm,
    up_pre_hbm,
    down_pre_hbm,
    query_hbm,
    forget_hbm,
    value_hbm,
    outgate_hbm,
    out_hbm,
    gate_post_hbm,
    up_post_hbm,
    down_post_hbm,
    state_hbm,
    layer_ref,
    next_ref,
    gate_pre,
    up_pre,
    down_pre,
    own_weights,
    plane_weights,
    out_weight,
    gate_post,
    up_post,
    down_post,
    state,
    state_half,
    gather_a,
    gather_b,
    wide_a,
    wide_b,
    spread,
    scaled_rows,
    columns_out,
    columns_landed,
    columns_in,
    rows_out,
    rows_in,
    stream_rows,
    proj_out,
    proj_in,
    inverse_rows,
    keep_t,
    inject_t,
    value_rows,
    mixed_rows,
    mixed_out,
    mixed_in,
    partial_b,
    landed_b,
    gate_up_out,
    gate_up_in,
    squares_out,
    squares_in,
    row_squares_out,
    row_squares_in,
    load_sem,
    send_sem,
    recv_sem,
    tp_send,
    tp_recv,
):
    me = lax.axis_index("kv")
    core = lax.axis_index("tp")
    rows, width = residual_ref.shape
    model = 2 * width
    total = n_kv * rows
    packed = rows * GROUPS
    planes = n_kv // PLANE
    half_planes = planes // 2
    depth_at, spot = me // PLANE, lax.rem(me, PLANE)
    spot_x, spot_y = lax.rem(spot, 2), spot // 2
    slot = lax.rem(me, GROUPS)
    holder = me // GROUPS == core
    f32, bf16 = jnp.float32, jnp.bfloat16

    def flipped(flip):
        return 2 * lax.rem(spot_y + flip // 2, 2) + lax.rem(spot_x + flip % 2, 2)

    def others():
        for step in sorted(range(planes), key=lambda s: -min(s, planes - s)):
            for flip in FLIPS:
                if step or flip:
                    yield lax.rem(depth_at + step, planes) * PLANE + flipped(flip)

    def load(index, source, target):
        return pltpu.make_async_copy(source, target, load_sem.at[index])

    loads = [
        load(0, forget_hbm, own_weights.at[0]),
        load(1, value_hbm, own_weights.at[1]),
        load(2, query_hbm, own_weights.at[2]),
        load(3, outgate_hbm, own_weights.at[3]),
        load(4, gate_pre_hbm, gate_pre),
        load(5, up_pre_hbm, up_pre),
        load(6, down_pre_hbm, down_pre),
        load(7, state_hbm, state),
        load(8, out_hbm, out_weight),
        load(9, gate_post_hbm, gate_post),
        load(10, up_post_hbm, up_post),
        load(11, down_post_hbm, down_post),
    ]
    for copy in loads:
        copy.start()

    def spread_rows(target, values):
        for group in range(GROUPS):
            target[pl.ds(group, values.shape[0], stride=GROUPS), :] = values[:, lanes(group)]

    residual = residual_ref[...].astype(f32)
    spread_rows(stream_rows, residual)
    gather_a[me] = stream_rows[...].astype(bf16)

    barrier = pltpu.get_barrier_semaphore()
    for peer in others():
        pl.semaphore_signal(
            barrier, inc=1, device_id={"kv": peer}, device_id_type=pl.DeviceIdType.MESH
        )
    pl.semaphore_signal(
        barrier, inc=1, device_id={"tp": 1 - core}, device_id_type=pl.DeviceIdType.MESH
    )
    pl.semaphore_wait(barrier, n_kv)

    def remote(exchange, source, target, **device):
        return pltpu.make_async_remote_copy(
            src_ref=source,
            dst_ref=target,
            send_sem=send_sem.at[exchange],
            recv_sem=recv_sem.at[exchange],
            device_id=device,
            device_id_type=pl.DeviceIdType.MESH,
        )

    def all_of(exchange, ref):
        return remote(exchange, ref, ref, tp=1 - core)

    def tp_copy(index, source, target):
        return pltpu.make_async_remote_copy(
            src_ref=source,
            dst_ref=target,
            send_sem=tp_send.at[index],
            recv_sem=tp_recv.at[index],
            device_id={"tp": 1 - core},
            device_id_type=pl.DeviceIdType.MESH,
        )

    def feed_forward(which, gathered, wide, gain_ref, gate, up, down):
        wide[...] = gathered[...].astype(f32).reshape(n_kv * packed, LANES)
        square_lanes = jnp.zeros((total, LANES), f32)
        for group in range(GROUPS):
            part = wide[pl.ds(group, total, stride=GROUPS), :]
            square_lanes += part * part
            scaled_rows[:, lanes(group)] = (part * gain_ref[:, lanes(group)]).astype(bf16)
        scaled = scaled_rows[...]
        squares = jnp.sum(square_lanes, axis=1, keepdims=True)
        squares_out[which] = jnp.broadcast_to(squares, squares_out.shape[1:])
        gate_part = dot_columns(scaled, gate[...])
        gate_up_out[which, 0] = gate_part.astype(bf16)
        copies = [
            tp_copy(3 * which, squares_out.at[which], squares_in.at[which]),
            tp_copy(3 * which + 1, gate_up_out.at[which, 0], gate_up_in.at[which, 0]),
            tp_copy(3 * which + 2, gate_up_out.at[which, 1], gate_up_in.at[which, 1]),
        ]
        copies[0].start()
        copies[1].start()
        up_part = dot_columns(scaled, up[...])
        gate_up_out[which, 1] = up_part.astype(bf16)
        copies[2].start()
        for copy in copies:
            copy.wait_recv()
        inverse = lax.rsqrt((squares + squares_in[which][:, 0:1]) / model + EPSILON)
        gate_sum = (gate_part + gate_up_in[which, 0].astype(f32)) * inverse
        up_sum = (up_part + gate_up_in[which, 1].astype(f32)) * inverse
        hidden = (gate_sum / (1.0 + jnp.exp(-gate_sum)) * up_sum).astype(bf16)
        return jnp.dot(hidden, down[...], preferred_element_type=f32), copies

    def gather_start(exchange, gathered):
        for peer in others():
            remote(exchange, gathered.at[me], gathered.at[me], kv=peer).start()

    def but_one(ref):
        return ref.at[pl.ds(0, n_kv - 1)]

    gather_start(GATHER_A, gather_a)
    for copy in loads[0:4]:
        copy.wait()
    for flip in FLIPS[:-1]:
        peer_spot = flipped(flip)
        remote(
            WEIGHTS,
            own_weights.at[peer_spot],
            plane_weights.at[spot],
            kv=depth_at * PLANE + peer_spot,
        ).start()
    plane_weights[spot] = own_weights[spot]
    mixed_rows[packed:, :] = jnp.zeros((mixed_rows.shape[0] - packed, LANES), f32)
    for copy in loads[4:7]:
        copy.wait()
    all_of(GATHER_A, but_one(gather_a)).wait_recv()
    branch_a, copies_a = feed_forward(
        0, gather_a, wide_a, gain_pre_ref, gate_pre, up_pre, down_pre
    )
    for group in range(GROUPS):
        columns_out[group] = branch_a[:, lanes(group)].astype(bf16)
    for flip in FLIPS:
        for step in range(half_planes - 1, -1, -1):
            plane = core * half_planes + lax.rem(depth_at + step, half_planes)
            peer = plane * PLANE + flipped(flip)
            copy = remote(
                SCATTER_A, columns_out.at[lax.rem(peer, GROUPS)], columns_landed.at[me], kv=peer
            )
            if step or flip:
                copy.start()
            else:
                pl.when(jnp.logical_not(holder))(copy.start)

    @pl.when(holder)
    def _():
        columns_landed[me] = columns_out[slot]
        all_of(SCATTER_A, but_one(columns_landed)).wait_recv()
        branch = jnp.sum(columns_landed[...].astype(f32), axis=0)
        shared = wide_a[pl.ds(slot, total, stride=GROUPS), :]
        stream = (shared + 0.5 * branch).astype(bf16).astype(f32)
        columns_in[spot] = (stream * gain_mix_ref[me]).astype(bf16)
        block = columns_in.at[spot]
        for flip in FLIPS:
            peer = depth_at * PLANE + flipped(flip)
            if flip:
                remote(SHARE, block, block, kv=peer, tp=core).start()
            remote(SHARE, block, block, kv=peer, tp=1 - core).start()
        for owner in range(n_kv):
            rows_out[owner] = stream[owner * rows : (owner + 1) * rows, :]
        for peer in others():
            remote(ROWS, rows_out.at[peer], rows_in.at[slot], kv=peer).start()
        rows_in[slot] = rows_out[me]
        all_of(SHARE, columns_in.at[pl.ds(0, PLANE - 1)]).wait_recv()

    @pl.when(jnp.logical_not(holder))
    def _():
        all_of(SHARE, columns_in).wait_recv()

    all_of(WEIGHTS, plane_weights.at[pl.ds(0, PLANE - 1)]).wait_recv()
    columns = jnp.concatenate([columns_in[part] for part in range(PLANE)], axis=1)
    product = jnp.dot(
        columns,
        plane_weights[...].reshape(PLANE * LANES, width),
        preferred_element_type=f32,
    )
    spread_rows(spread, product)
    proj_out[...] = spread[...].astype(bf16).reshape(n_kv, packed, LANES)
    for peer in others():
        remote(PROJECT, proj_out.at[peer], proj_in.at[me], kv=peer).start()
    proj_in[me] = proj_out[me]

    @pl.when(holder)
    def _():
        all_of(ROWS, rows_in.at[pl.ds(0, GROUPS - 1)]).wait_recv()

    @pl.when(jnp.logical_not(holder))
    def _():
        all_of(ROWS, rows_in).wait_recv()

    for group in range(GROUPS):
        stream_rows[pl.ds(group, rows, stride=GROUPS), :] = rows_in[group]
    stream = stream_rows[...].reshape(rows, GROUPS, LANES)
    row_squares = jnp.sum(stream * stream, axis=1)
    row_squares_out[...] = row_squares
    square_copy = tp_copy(6, row_squares_out, row_squares_in)
    square_copy.start()
    loads[7].wait()
    for row in range(rows):
        for head in range(GROUPS):
            state_half[row // 2, head * LANES : (head + 1) * LANES, lanes(row % 2)] = state[
                row, head
            ].astype(bf16)
    square_copy.wait_recv()
    squares = jnp.sum(row_squares + row_squares_in[...], axis=1, keepdims=True)
    inverse = lax.rsqrt(squares / model + EPSILON)
    for row in range(rows):
        inverse_rows[row * GROUPS : (row + 1) * GROUPS, :] = jnp.broadcast_to(
            inverse[row : row + 1, :], (GROUPS, LANES)
        )
    loads[8].wait()
    all_of(PROJECT, but_one(proj_in)).wait_recv()

    def projected(index):
        parts = [proj_in[plane * PLANE + index].astype(f32) for plane in range(planes)]
        return sum(parts[1:], parts[0]) * inverse_rows[...]

    floor_rate = jnp.concatenate([lower_ref[...]] * rows, axis=0)
    forget_pre = projected(0)
    keep = floor_rate + (1.0 - floor_rate) / (1.0 + jnp.exp(-forget_pre))
    inject = (1.0 - floor_rate) / (1.0 + jnp.exp(forget_pre))
    query_pre = projected(2)
    query = query_pre / (1.0 + jnp.exp(-query_pre))
    value = projected(1)
    value_rows[...] = value
    weighted = query * keep
    direct = jnp.sum(query * inject, axis=1, keepdims=True) * value
    head_index = lax.broadcasted_iota(jnp.int32, (GROUPS, LANES), 0)
    read = []
    for pair in range(rows // 2):
        diagonal = []
        for row in (2 * pair, 2 * pair + 1):
            heads = weighted[row * GROUPS : (row + 1) * GROUPS, :]
            diagonal.append(
                jnp.concatenate(
                    [jnp.where(head_index == head, heads, 0.0) for head in range(GROUPS)], axis=1
                )
            )
        both = jnp.dot(
            jnp.concatenate(diagonal, axis=0).astype(bf16),
            state_half[pair],
            preferred_element_type=f32,
        )
        read.append(both[0:GROUPS, lanes(0)])
        read.append(both[GROUPS : 2 * GROUPS, lanes(1)])
    readout = jnp.concatenate(read, axis=0) + direct
    outgate_pre = projected(3)
    outgate = outgate_pre / (1.0 + jnp.exp(-outgate_pre))
    scale = lax.rsqrt(jnp.mean(readout * readout, axis=1, keepdims=True) + EPSILON)
    head_gain = jnp.concatenate([head_gain_ref[...]] * rows, axis=0)
    mixed_rows[0:packed, :] = readout * scale * head_gain * outgate
    mixed_heads = jnp.concatenate(
        [mixed_rows[pl.ds(head, GROUPS, stride=GROUPS), :] for head in range(GROUPS)], axis=1
    ).astype(bf16)
    mixed_part = jnp.dot(mixed_heads, out_weight[...], preferred_element_type=f32)[0:rows]
    for half in range(2):
        spread_rows(mixed_out.at[half], mixed_part[:, half * width : (half + 1) * width])
    mixed_copy = tp_copy(7, mixed_out.at[1 - core], mixed_in)
    mixed_copy.start()
    for row in range(rows):
        span = slice(row * GROUPS, (row + 1) * GROUPS)
        keep_t[row] = keep[span].T
        inject_t[row] = inject[span].T
    mixed_copy.wait_recv()
    stream_b = (stream_rows[...] + (mixed_out[core] + mixed_in[...])).astype(bf16)
    gather_b[me] = stream_b
    gather_start(GATHER_B, gather_b)

    def update(row, carry):
        keep_columns = keep_t[row]
        inject_columns = inject_t[row]
        for head in range(GROUPS):
            column = slice(head, head + 1)
            values = value_rows[pl.ds(row * GROUPS + head, 1), :]
            next_ref[row, head] = (
                keep_columns[:, column] * state[row, head] + inject_columns[:, column] * values
            )
        return carry

    lax.fori_loop(0, rows, update, 0)
    for copy in loads[9:12]:
        copy.wait()
    all_of(GATHER_B, but_one(gather_b)).wait_recv()
    branch_b, copies_b = feed_forward(
        1, gather_b, wide_b, gain_post_ref, gate_post, up_post, down_post
    )
    spread_rows(spread, branch_b)
    partial_b[...] = spread[...].astype(bf16).reshape(n_kv, packed, LANES)
    for peer in others():
        remote(SCATTER_B, partial_b.at[peer], landed_b.at[me], kv=peer).start()
    landed_b[me] = partial_b[me]
    for copy in copies_a + copies_b + [square_copy, mixed_copy]:
        copy.wait_send()
    all_of(GATHER_A, but_one(gather_a)).wait_send()
    all_of(WEIGHTS, plane_weights.at[pl.ds(0, PLANE - 1)]).wait_send()
    all_of(PROJECT, but_one(proj_out)).wait_send()
    all_of(GATHER_B, but_one(gather_b)).wait_send()

    @pl.when(holder)
    def _():
        all_of(SCATTER_A, columns_out.at[pl.ds(0, GROUPS - 1)]).wait_send()
        all_of(SHARE, columns_landed.at[pl.ds(0, 2 * PLANE - 1)]).wait_send()
        all_of(ROWS, but_one(rows_out)).wait_send()

    @pl.when(jnp.logical_not(holder))
    def _():
        all_of(SCATTER_A, columns_out).wait_send()

    all_of(SCATTER_B, but_one(landed_b)).wait_recv()
    branch = jnp.sum(landed_b[...].astype(f32), axis=0)
    spread[0:packed, :] = gather_b[me].astype(f32) + 0.5 * branch
    for group in range(GROUPS):
        layer_ref[:, lanes(group)] = spread[pl.ds(group, rows, stride=GROUPS), :].astype(bf16)
    all_of(SCATTER_B, but_one(partial_b)).wait_send()


def store_results(layer_in, state_in, layer_out, state_out, sem):
    copies = [pltpu.make_async_copy(layer_in, layer_out, sem.at[0])]
    for row in range(state_in.shape[0]):
        copies.append(pltpu.make_async_copy(state_in.at[row], state_out.at[row], sem.at[1 + row]))
    for copy in copies:
        copy.start()
    for copy in copies:
        copy.wait()


def fused_shards(
    n_kv,
    residual_in,
    gain_pre,
    gate_pre,
    up_pre,
    down_pre,
    gain_mix,
    query_weight,
    forget_weight,
    value_weight,
    outgate_weight,
    lower_bound,
    head_gain,
    out_weight,
    gain_post,
    gate_post,
    up_post,
    down_post,
    memory_state,
):
    rows, width = residual_in.shape
    hidden = gate_pre.shape[1]
    total = n_kv * rows
    packed = rows * GROUPS
    f32, bf16 = jnp.float32, jnp.bfloat16
    vmem = pl.BlockSpec(memory_space=pltpu.VMEM)
    hbm = pl.BlockSpec(memory_space=pltpu.HBM)
    like = lambda array: pltpu.VMEM(array.shape, array.dtype)
    blocks = lambda: pltpu.VMEM((n_kv, packed, LANES), bf16)
    outs = (
        jax.ShapeDtypeStruct(residual_in.shape, residual_in.dtype),
        jax.ShapeDtypeStruct(memory_state.shape, memory_state.dtype),
    )
    layer, state = pl.pallas_call(
        functools.partial(fused_layer, n_kv),
        out_shape=tuple(pltpu.VMEM(out.shape, out.dtype) for out in outs),
        in_specs=[vmem] * 6 + [hbm] * 12,
        out_specs=(vmem, vmem),
        scratch_shapes=[
            pltpu.VMEM((hidden, width), bf16),
            pltpu.VMEM((hidden, width), bf16),
            like(down_pre),
            pltpu.VMEM((PLANE,) + query_weight.shape, bf16),
            pltpu.VMEM((PLANE,) + query_weight.shape, bf16),
            like(out_weight),
            pltpu.VMEM((hidden, width), bf16),
            pltpu.VMEM((hidden, width), bf16),
            like(down_post),
            like(memory_state),
            pltpu.VMEM((rows // 2, width, 2 * LANES), bf16),
            blocks(),
            blocks(),
            pltpu.VMEM((n_kv * packed, LANES), f32),
            pltpu.VMEM((n_kv * packed, LANES), f32),
            pltpu.VMEM((n_kv * packed, LANES), f32),
            pltpu.VMEM((total, width), bf16),
            pltpu.VMEM((GROUPS, total, LANES), bf16),
            pltpu.VMEM((n_kv, total, LANES), bf16),
            pltpu.VMEM((PLANE, total, LANES), bf16),
            pltpu.VMEM((n_kv, rows, LANES), f32),
            pltpu.VMEM((GROUPS, rows, LANES), f32),
            pltpu.VMEM((packed, LANES), f32),
            blocks(),
            blocks(),
            pltpu.VMEM((packed, LANES), f32),
            pltpu.VMEM((rows, LANES, GROUPS), f32),
            pltpu.VMEM((rows, LANES, GROUPS), f32),
            pltpu.VMEM((packed, LANES), f32),
            pltpu.VMEM((GROUPS * GROUPS, LANES), f32),
            pltpu.VMEM((2, packed, LANES), f32),
            pltpu.VMEM((packed, LANES), f32),
            blocks(),
            blocks(),
            pltpu.VMEM((2, 2, total, hidden), bf16),
            pltpu.VMEM((2, 2, total, hidden), bf16),
            pltpu.VMEM((2, total, LANES), f32),
            pltpu.VMEM((2, total, LANES), f32),
            pltpu.VMEM((rows, LANES), f32),
            pltpu.VMEM((rows, LANES), f32),
            pltpu.SemaphoreType.DMA((12,)),
            pltpu.SemaphoreType.DMA((EXCHANGES,)),
            pltpu.SemaphoreType.DMA((EXCHANGES,)),
            pltpu.SemaphoreType.DMA((8,)),
            pltpu.SemaphoreType.DMA((8,)),
        ],
        compiler_params=pltpu.CompilerParams(
            collective_id=0, has_side_effects=True, vmem_limit_bytes=56 * 1024 * 1024
        ),
    )(
        residual_in,
        gain_pre.reshape(1, width),
        gain_mix.reshape(n_kv, 1, LANES),
        lower_bound.reshape(GROUPS, LANES),
        head_gain.reshape(GROUPS, LANES),
        gain_post.reshape(1, width),
        gate_pre.T,
        up_pre.T,
        down_pre,
        query_weight,
        forget_weight,
        value_weight,
        outgate_weight,
        out_weight,
        gate_post.T,
        up_post.T,
        down_post,
        memory_state,
    )
    return pl.pallas_call(
        store_results,
        out_shape=outs,
        in_specs=[vmem, vmem],
        out_specs=(hbm, hbm),
        scratch_shapes=[pltpu.SemaphoreType.DMA((1 + rows,))],
        compiler_params=pltpu.CompilerParams(vmem_limit_bytes=8 * 1024 * 1024),
    )(layer, state)


def solution(mesh):
    n_kv, n_tp = mesh.shape["kv"], mesh.shape["tp"]
    fits = n_tp == 2 and n_kv * LANES == D and n_kv // n_tp == GROUPS
    body = functools.partial(fused_shards, n_kv) if fits else shards
    in_specs = (
        P("kv", "tp"),
        P("tp"),
        P("tp", "kv"),
        P("tp", "kv"),
        P("kv", "tp"),
        P(),
        P("kv", "tp"),
        P("kv", "tp"),
        P("kv", "tp"),
        P("kv", "tp"),
        P("tp"),
        P("tp"),
        P("tp", None),
        P("tp"),
        P("tp", "kv"),
        P("tp", "kv"),
        P("kv", "tp"),
        P("kv", "tp", None, None),
    )
    out_specs = (P("kv", "tp"), P("kv", "tp", None, None))
    return jax.shard_map(body, mesh=mesh, in_specs=in_specs, out_specs=out_specs, check_vma=False)
```

```python
import functools

import jax
import jax.numpy as jnp
from jax import lax
from jax.experimental import pallas as pl
from jax.experimental.pallas import tpu as pltpu
from jax.sharding import PartitionSpec as P

D = 2048
HEAD_DIM = 128


EPSILON = 1e-06


def channel_mixer(row_block, gain_vec, gate_weight, up_weight, down_weight):
    gathered = lax.all_gather(row_block, "kv", axis=0, tiled=True)
    widened = gathered.astype(jnp.float32)
    part_squares = jnp.sum(widened * widened, axis=1)
    scaled = (widened * gain_vec).astype(jnp.bfloat16)
    gate_part = jnp.dot(scaled, gate_weight, preferred_element_type=jnp.float32)
    up_part = jnp.dot(scaled, up_weight, preferred_element_type=jnp.float32)
    gate_share, up_share, square_share = (
        lax.psum_scatter(
            gate_part.astype(jnp.bfloat16), "tp", scatter_dimension=0, tiled=True
        ).astype(jnp.float32),
        lax.psum_scatter(
            up_part.astype(jnp.bfloat16), "tp", scatter_dimension=0, tiled=True
        ).astype(jnp.float32),
        lax.psum_scatter(
            part_squares.astype(jnp.bfloat16), "tp", scatter_dimension=0, tiled=True
        ).astype(jnp.float32),
    )
    share_inverse = lax.rsqrt(square_share / D + EPSILON)[:, None]
    hidden_share = (jax.nn.silu(gate_share * share_inverse) * (up_share * share_inverse)).astype(
        jnp.bfloat16
    )
    hidden = lax.all_gather(hidden_share, "tp", axis=0, tiled=True)
    return lax.psum_scatter(
        jnp.dot(hidden, down_weight, preferred_element_type=jnp.float32),
        "kv",
        scatter_dimension=0,
        tiled=True,
    )


def token_mixer(
    stream_a,
    gain_mix,
    query_weight,
    forget_weight,
    value_weight,
    outgate_weight,
    lower_bound,
    head_gain,
    out_weight,
    memory_state,
):
    full_rows = lax.all_gather(stream_a, "tp", axis=1, tiled=True)
    widened = full_rows.astype(jnp.float32)
    inverse = lax.rsqrt(jnp.mean(widened * widened, axis=1, keepdims=True) + EPSILON)
    scaled = (widened * gain_mix).astype(jnp.bfloat16)
    weights = (query_weight, forget_weight, value_weight, outgate_weight)
    blocks = lax.all_to_all(scaled, "kv", split_axis=1, concat_axis=0, tiled=True)
    joined = jnp.concatenate(weights, axis=1)
    projected = lax.psum_scatter(
        jnp.dot(blocks, joined, preferred_element_type=jnp.float32),
        "kv",
        scatter_dimension=0,
        tiled=True,
    )
    projected = projected * inverse
    seq_rows = scaled.shape[0]
    local_heads = query_weight.shape[1] // HEAD_DIM
    reshaped = projected.reshape(seq_rows, 4, local_heads, HEAD_DIM)
    query_pre = reshaped[:, 0]
    forget_pre = reshaped[:, 1]
    value_pre = reshaped[:, 2]
    outgate_pre = reshaped[:, 3]
    floor_rate = lower_bound.reshape(local_heads, HEAD_DIM)
    log_keep = jnp.logaddexp(
        jnp.log(floor_rate), jnp.log1p(-floor_rate) + jax.nn.log_sigmoid(forget_pre)
    )
    inject = (1.0 - floor_rate) * jax.nn.sigmoid(-forget_pre)
    next_state = (
        jnp.exp(log_keep)[..., None] * memory_state + inject[..., None] * value_pre[:, :, None, :]
    )
    readout = jnp.einsum(
        "bhk,bhkv->bhv", jax.nn.silu(query_pre), next_state, precision=lax.Precision.HIGHEST
    )
    normed = (
        readout
        * lax.rsqrt(jnp.mean(readout * readout, axis=2, keepdims=True) + EPSILON)
        * head_gain.reshape(local_heads, HEAD_DIM)
    )
    mixed_heads = (
        (normed * jax.nn.silu(outgate_pre))
        .reshape(seq_rows, local_heads * HEAD_DIM)
        .astype(jnp.bfloat16)
    )
    partial_out = jnp.dot(mixed_heads, out_weight, preferred_element_type=jnp.float32)
    mixed = lax.psum_scatter(
        partial_out.astype(jnp.bfloat16), "tp", scatter_dimension=1, tiled=True
    ).astype(jnp.float32)
    return (mixed, next_state)


def shards(
    residual_in,
    gain_pre,
    gate_pre,
    up_pre,
    down_pre,
    gain_mix,
    query_weight,
    forget_weight,
    value_weight,
    outgate_weight,
    lower_bound,
    head_gain,
    out_weight,
    gain_post,
    gate_post,
    up_post,
    down_post,
    memory_state,
):
    branch_a = channel_mixer(residual_in, gain_pre, gate_pre, up_pre, down_pre)
    stream_a = (residual_in.astype(jnp.float32) + 0.5 * branch_a).astype(jnp.bfloat16)
    mixed, next_state = token_mixer(
        stream_a,
        gain_mix,
        query_weight,
        forget_weight,
        value_weight,
        outgate_weight,
        lower_bound,
        head_gain,
        out_weight,
        memory_state,
    )
    stream_b = (stream_a.astype(jnp.float32) + mixed).astype(jnp.bfloat16)
    branch_b = channel_mixer(stream_b, gain_post, gate_post, up_post, down_post)
    layer_out = (stream_b.astype(jnp.float32) + 0.5 * branch_b).astype(jnp.bfloat16)
    return (layer_out, next_state)


LANES = 128
GROUPS = 8
PLANE = 4
GATHER_A, WEIGHTS, SCATTER_A, SHARE, ROWS, PROJECT, GATHER_B, SCATTER_B = range(8)
EXCHANGES = 8
HOLDER = 1
FLIPS = (3, 1, 2, 0)


def lanes(group):
    return slice(group * LANES, (group + 1) * LANES)


def fused_layer(
    n_kv,
    residual_ref,
    gain_pre_ref,
    gain_mix_ref,
    lower_ref,
    head_gain_ref,
    gain_post_ref,
    gate_pre_hbm,
    up_pre_hbm,
    down_pre_hbm,
    query_hbm,
    forget_hbm,
    value_hbm,
    outgate_hbm,
    out_hbm,
    gate_post_hbm,
    up_post_hbm,
    down_post_hbm,
    state_hbm,
    layer_ref,
    next_ref,
    gate_pre,
    up_pre,
    down_pre,
    own_weights,
    plane_weights,
    out_weight,
    gate_post,
    up_post,
    down_post,
    gate_pre_t,
    up_pre_t,
    gate_post_t,
    up_post_t,
    state,
    state_half,
    gather_a,
    gather_b,
    wide_a,
    wide_b,
    spread,
    scaled_rows,
    columns_out,
    columns_landed,
    columns_in,
    shared_out,
    shared_in,
    rows_out,
    rows_in,
    stream_rows,
    proj_out,
    proj_in,
    inverse_rows,
    keep_t,
    inject_t,
    value_rows,
    mixed_rows,
    mixed_out,
    mixed_own,
    mixed_in,
    partial_b,
    landed_b,
    gate_up_out,
    gate_up_in,
    squares_out,
    squares_in,
    row_squares_out,
    row_squares_in,
    load_sem,
    send_sem,
    recv_sem,
    tp_send,
    tp_recv,
):
    me = lax.axis_index("kv")
    core = lax.axis_index("tp")
    rows, width = residual_ref.shape
    model = 2 * width
    total = n_kv * rows
    packed = rows * GROUPS
    planes = n_kv // PLANE
    half_planes = planes // 2
    depth_at, spot = me // PLANE, lax.rem(me, PLANE)
    spot_x, spot_y = lax.rem(spot, 2), spot // 2
    slot = lax.rem(me, GROUPS)
    owner_core = me // GROUPS
    holder = core == HOLDER
    owns = jnp.logical_and(holder, owner_core == HOLDER)
    f32, bf16 = jnp.float32, jnp.bfloat16

    def flipped(flip):
        return 2 * lax.rem(spot_y + flip // 2, 2) + lax.rem(spot_x + flip % 2, 2)

    def others():
        for flip in FLIPS:
            for step in range(planes - 1, -1, -1):
                plane = 2 * lax.rem(depth_at // 2 + step // 2, 2) + lax.rem(depth_at + step, 2)
                if step or flip:
                    yield plane * PLANE + flipped(flip)

    def load(index, source, target):
        return pltpu.make_async_copy(source, target, load_sem.at[index])

    loads = [
        load(0, forget_hbm, own_weights.at[0]),
        load(1, value_hbm, own_weights.at[1]),
        load(2, query_hbm, own_weights.at[2]),
        load(3, outgate_hbm, own_weights.at[3]),
        load(4, gate_pre_hbm, gate_pre),
        load(5, up_pre_hbm, up_pre),
        load(6, down_pre_hbm, down_pre),
        load(7, state_hbm, state),
        load(8, out_hbm.at[:, pl.ds(0, width)], out_weight.at[0]),
        load(12, out_hbm.at[:, pl.ds(width, width)], out_weight.at[1]),
        load(9, gate_post_hbm, gate_post),
        load(10, up_post_hbm, up_post),
        load(11, down_post_hbm, down_post),
    ]
    for copy in loads:
        copy.start()

    def spread_rows(target, values):
        for group in range(GROUPS):
            target[pl.ds(group, values.shape[0], stride=GROUPS), :] = values[:, lanes(group)]

    residual = residual_ref[...].astype(f32)
    spread_rows(stream_rows, residual)
    gather_a[me] = stream_rows[...].astype(bf16)

    barrier = pltpu.get_barrier_semaphore()
    for peer in others():
        pl.semaphore_signal(
            barrier, inc=1, device_id={"kv": peer}, device_id_type=pl.DeviceIdType.MESH
        )
    pl.semaphore_signal(
        barrier, inc=1, device_id={"tp": 1 - core}, device_id_type=pl.DeviceIdType.MESH
    )
    pl.semaphore_wait(barrier, n_kv)

    def remote(exchange, source, target, **device):
        return pltpu.make_async_remote_copy(
            src_ref=source,
            dst_ref=target,
            send_sem=send_sem.at[exchange],
            recv_sem=recv_sem.at[exchange],
            device_id=device,
            device_id_type=pl.DeviceIdType.MESH,
        )

    def all_of(exchange, ref):
        return remote(exchange, ref, ref, tp=1 - core)

    def tp_copy(index, source, target):
        return pltpu.make_async_remote_copy(
            src_ref=source,
            dst_ref=target,
            send_sem=tp_send.at[index],
            recv_sem=tp_recv.at[index],
            device_id={"tp": 1 - core},
            device_id_type=pl.DeviceIdType.MESH,
        )

    def feed_forward(which, gathered, wide, gain_ref, gate, up, down):
        wide[...] = gathered[...].astype(f32).reshape(n_kv * packed, LANES)
        square_lanes = jnp.zeros((total, LANES), f32)
        for group in range(GROUPS):
            part = wide[pl.ds(group, total, stride=GROUPS), :]
            square_lanes += part * part
            scaled_rows[:, lanes(group)] = (part * gain_ref[:, lanes(group)]).astype(bf16)
        scaled = scaled_rows[...]
        squares = jnp.sum(square_lanes, axis=1, keepdims=True)
        squares_out[which] = jnp.broadcast_to(squares, squares_out.shape[1:])
        gate_part = jnp.dot(scaled, gate[...], preferred_element_type=f32)
        gate_up_out[which, 0] = gate_part.astype(bf16)
        copies = [
            tp_copy(3 * which, squares_out.at[which], squares_in.at[which]),
            tp_copy(3 * which + 1, gate_up_out.at[which, 0], gate_up_in.at[which, 0]),
            tp_copy(3 * which + 2, gate_up_out.at[which, 1], gate_up_in.at[which, 1]),
        ]
        copies[0].start()
        copies[1].start()
        up_part = jnp.dot(scaled, up[...], preferred_element_type=f32)
        gate_up_out[which, 1] = up_part.astype(bf16)
        copies[2].start()
        for copy in copies:
            copy.wait_recv()
        inverse = lax.rsqrt((squares + squares_in[which][:, 0:1]) / model + EPSILON)
        gate_sum = (gate_part + gate_up_in[which, 0].astype(f32)) * inverse
        up_sum = (up_part + gate_up_in[which, 1].astype(f32)) * inverse
        hidden = (gate_sum / (1.0 + jnp.exp(-gate_sum)) * up_sum).astype(bf16)
        return jnp.dot(hidden, down[...], preferred_element_type=f32), copies

    def gather_start(exchange, gathered):
        for peer in others():
            remote(exchange, gathered.at[me], gathered.at[me], kv=peer).start()

    def turn(target, source):
        for group in range(GROUPS):
            target[lanes(group), :] = source[:, lanes(group)].T

    def but_one(ref):
        return ref.at[pl.ds(0, n_kv - 1)]

    gather_start(GATHER_A, gather_a)
    for copy in loads[0:4]:
        copy.wait()
    for flip in FLIPS[:-1]:
        peer_spot = flipped(flip)
        remote(
            WEIGHTS,
            own_weights.at[peer_spot],
            plane_weights.at[spot],
            kv=depth_at * PLANE + peer_spot,
        ).start()
    plane_weights[spot] = own_weights[spot]
    mixed_rows[packed:, :] = jnp.zeros((mixed_rows.shape[0] - packed, LANES), f32)
    for copy in loads[4:7]:
        copy.wait()
    turn(gate_pre_t, gate_pre)
    turn(up_pre_t, up_pre)
    all_of(GATHER_A, but_one(gather_a)).wait_recv()
    branch_a, copies_a = feed_forward(
        0, gather_a, wide_a, gain_pre_ref, gate_pre_t, up_pre_t, down_pre
    )
    for group in range(GROUPS):
        columns_out[group] = branch_a[:, lanes(group)].astype(bf16)
    shared_copy = tp_copy(8, shared_out, shared_in)

    @pl.when(owner_core == core)
    def _():
        shared_out[...] = wide_a[pl.ds(slot, total, stride=GROUPS), :].astype(bf16)

        @pl.when(jnp.logical_not(holder))
        def _():
            shared_copy.start()

    for flip in FLIPS:
        for step in range(half_planes - 1, -1, -1):
            plane = core * half_planes + lax.rem(depth_at + step, half_planes)
            peer = plane * PLANE + flipped(flip)
            copy = remote(
                SCATTER_A,
                columns_out.at[lax.rem(peer, GROUPS)],
                columns_landed.at[me],
                kv=peer,
                tp=HOLDER,
            )
            if step or flip:
                copy.start()
            else:
                pl.when(jnp.logical_not(owns))(copy.start)

    @pl.when(holder)
    def _():
        @pl.when(owns)
        def _():
            columns_landed[me] = columns_out[slot]
            all_of(SCATTER_A, but_one(columns_landed)).wait_recv()
            shared_in[...] = shared_out[...]

        @pl.when(jnp.logical_not(owns))
        def _():
            all_of(SCATTER_A, columns_landed).wait_recv()
            shared_copy.wait_recv()

        branch = jnp.sum(columns_landed[...].astype(f32), axis=0)
        stream = (shared_in[...].astype(f32) + 0.5 * branch).astype(bf16).astype(f32)
        columns_in[spot] = (stream * gain_mix_ref[me]).astype(bf16)
        block = columns_in.at[spot]
        for flip in FLIPS:
            peer = depth_at * PLANE + flipped(flip)
            remote(SHARE, block, block, kv=peer, tp=1 - core).start()
            if flip:
                remote(SHARE, block, block, kv=peer, tp=core).start()
        for owner in range(n_kv):
            rows_out[owner] = stream[owner * rows : (owner + 1) * rows, :]
        for peer in others():
            remote(ROWS, rows_out.at[peer], rows_in.at[slot], kv=peer, tp=owner_core).start()

        @pl.when(owns)
        def _():
            rows_in[slot] = rows_out[me]

        @pl.when(jnp.logical_not(owns))
        def _():
            remote(ROWS, rows_out.at[me], rows_in.at[slot], tp=1 - core).start()

        all_of(SHARE, columns_in.at[pl.ds(0, PLANE - 1)]).wait_recv()

    @pl.when(jnp.logical_not(holder))
    def _():
        all_of(SHARE, columns_in).wait_recv()

    all_of(WEIGHTS, plane_weights.at[pl.ds(0, PLANE - 1)]).wait_recv()
    columns = jnp.concatenate([columns_in[part] for part in range(PLANE)], axis=1)
    product = jnp.dot(
        columns,
        plane_weights[...].reshape(PLANE * LANES, width),
        preferred_element_type=f32,
    )
    spread_rows(spread, product)
    proj_out[...] = spread[...].astype(bf16).reshape(n_kv, packed, LANES)
    for peer in others():
        remote(PROJECT, proj_out.at[peer], proj_in.at[me], kv=peer).start()
    proj_in[me] = proj_out[me]

    @pl.when(owns)
    def _():
        all_of(ROWS, rows_in.at[pl.ds(0, GROUPS - 1)]).wait_recv()

    @pl.when(jnp.logical_not(owns))
    def _():
        all_of(ROWS, rows_in).wait_recv()

    for group in range(GROUPS):
        stream_rows[pl.ds(group, rows, stride=GROUPS), :] = rows_in[group]
    stream = stream_rows[...].reshape(rows, GROUPS, LANES)
    row_squares = jnp.sum(stream * stream, axis=1)
    row_squares_out[...] = row_squares
    square_copy = tp_copy(6, row_squares_out, row_squares_in)
    square_copy.start()
    loads[7].wait()
    for row in range(rows):
        for head in range(GROUPS):
            state_half[row // 2, head * LANES : (head + 1) * LANES, lanes(row % 2)] = state[
                row, head
            ].astype(bf16)
    for copy in loads[10:12]:
        copy.wait()
    turn(gate_post_t, gate_post)
    turn(up_post_t, up_post)
    square_copy.wait_recv()
    squares = jnp.sum(row_squares + row_squares_in[...], axis=1, keepdims=True)
    inverse = lax.rsqrt(squares / model + EPSILON)
    for row in range(rows):
        inverse_rows[row * GROUPS : (row + 1) * GROUPS, :] = jnp.broadcast_to(
            inverse[row : row + 1, :], (GROUPS, LANES)
        )
    loads[8].wait()
    loads[9].wait()
    all_of(PROJECT, but_one(proj_in)).wait_recv()

    def projected(index):
        parts = [proj_in[plane * PLANE + index].astype(f32) for plane in range(planes)]
        return sum(parts[1:], parts[0]) * inverse_rows[...]

    floor_rate = jnp.concatenate([lower_ref[...]] * rows, axis=0)
    forget_pre = projected(0)
    keep = floor_rate + (1.0 - floor_rate) / (1.0 + jnp.exp(-forget_pre))
    inject = (1.0 - floor_rate) / (1.0 + jnp.exp(forget_pre))
    query_pre = projected(2)
    query = query_pre / (1.0 + jnp.exp(-query_pre))
    value = projected(1)
    value_rows[...] = value
    weighted = query * keep
    direct = jnp.sum(query * inject, axis=1, keepdims=True) * value
    head_index = lax.broadcasted_iota(jnp.int32, (GROUPS, LANES), 0)
    read = []
    for pair in range(rows // 2):
        diagonal = []
        for row in (2 * pair, 2 * pair + 1):
            heads = weighted[row * GROUPS : (row + 1) * GROUPS, :]
            diagonal.append(
                jnp.concatenate(
                    [jnp.where(head_index == head, heads, 0.0) for head in range(GROUPS)], axis=1
                )
            )
        both = jnp.dot(
            jnp.concatenate(diagonal, axis=0).astype(bf16),
            state_half[pair],
            preferred_element_type=f32,
        )
        read.append(both[0:GROUPS, lanes(0)])
        read.append(both[GROUPS : 2 * GROUPS, lanes(1)])
    readout = jnp.concatenate(read, axis=0) + direct
    outgate_pre = projected(3)
    outgate = outgate_pre / (1.0 + jnp.exp(-outgate_pre))
    scale = lax.rsqrt(jnp.mean(readout * readout, axis=1, keepdims=True) + EPSILON)
    head_gain = jnp.concatenate([head_gain_ref[...]] * rows, axis=0)
    mixed_rows[0:packed, :] = readout * scale * head_gain * outgate
    mixed_heads = jnp.concatenate(
        [mixed_rows[pl.ds(head, GROUPS, stride=GROUPS), :] for head in range(GROUPS)], axis=1
    ).astype(bf16)
    away = jnp.dot(mixed_heads, out_weight[1 - core], preferred_element_type=f32)
    spread_rows(mixed_out, away[0:rows])
    mixed_copy = tp_copy(7, mixed_out, mixed_in)
    mixed_copy.start()
    home = jnp.dot(mixed_heads, out_weight[core], preferred_element_type=f32)
    spread_rows(mixed_own, home[0:rows])
    for row in range(rows):
        span = slice(row * GROUPS, (row + 1) * GROUPS)
        keep_t[row] = keep[span].T
        inject_t[row] = inject[span].T
    mixed_copy.wait_recv()
    stream_b = (stream_rows[...] + (mixed_own[...] + mixed_in[...])).astype(bf16)
    gather_b[me] = stream_b
    gather_start(GATHER_B, gather_b)

    def update(row, carry):
        keep_columns = keep_t[row]
        inject_columns = inject_t[row]
        for head in range(GROUPS):
            column = slice(head, head + 1)
            values = value_rows[pl.ds(row * GROUPS + head, 1), :]
            next_ref[row, head] = (
                keep_columns[:, column] * state[row, head] + inject_columns[:, column] * values
            )
        return carry

    lax.fori_loop(0, rows, update, 0)
    loads[12].wait()
    all_of(GATHER_B, but_one(gather_b)).wait_recv()
    branch_b, copies_b = feed_forward(
        1, gather_b, wide_b, gain_post_ref, gate_post_t, up_post_t, down_post
    )
    spread_rows(spread, branch_b)
    partial_b[...] = spread[...].astype(bf16).reshape(n_kv, packed, LANES)
    for peer in others():
        remote(SCATTER_B, partial_b.at[peer], landed_b.at[me], kv=peer).start()
    landed_b[me] = partial_b[me]
    for copy in copies_a + copies_b + [square_copy, mixed_copy]:
        copy.wait_send()
    all_of(GATHER_A, but_one(gather_a)).wait_send()
    all_of(WEIGHTS, plane_weights.at[pl.ds(0, PLANE - 1)]).wait_send()
    all_of(PROJECT, but_one(proj_out)).wait_send()
    all_of(GATHER_B, but_one(gather_b)).wait_send()

    @pl.when(holder)
    def _():
        all_of(SHARE, columns_landed.at[pl.ds(0, 2 * PLANE - 1)]).wait_send()

    @pl.when(owns)
    def _():
        all_of(SCATTER_A, columns_out.at[pl.ds(0, GROUPS - 1)]).wait_send()
        all_of(ROWS, but_one(rows_out)).wait_send()

    @pl.when(jnp.logical_not(owns))
    def _():
        all_of(SCATTER_A, columns_out).wait_send()

        @pl.when(holder)
        def _():
            all_of(ROWS, rows_out).wait_send()

    @pl.when(jnp.logical_and(owner_core == core, jnp.logical_not(holder)))
    def _():
        shared_copy.wait_send()

    all_of(SCATTER_B, but_one(landed_b)).wait_recv()
    branch = jnp.sum(landed_b[...].astype(f32), axis=0)
    spread[0:packed, :] = gather_b[me].astype(f32) + 0.5 * branch
    for group in range(GROUPS):
        layer_ref[:, lanes(group)] = spread[pl.ds(group, rows, stride=GROUPS), :].astype(bf16)
    all_of(SCATTER_B, but_one(partial_b)).wait_send()


def store_results(layer_in, state_in, layer_out, state_out, sem):
    copies = [pltpu.make_async_copy(layer_in, layer_out, sem.at[0])]
    for row in range(state_in.shape[0]):
        copies.append(pltpu.make_async_copy(state_in.at[row], state_out.at[row], sem.at[1 + row]))
    for copy in copies:
        copy.start()
    for copy in copies:
        copy.wait()


def fused_shards(
    n_kv,
    residual_in,
    gain_pre,
    gate_pre,
    up_pre,
    down_pre,
    gain_mix,
    query_weight,
    forget_weight,
    value_weight,
    outgate_weight,
    lower_bound,
    head_gain,
    out_weight,
    gain_post,
    gate_post,
    up_post,
    down_post,
    memory_state,
):
    rows, width = residual_in.shape
    hidden = gate_pre.shape[1]
    total = n_kv * rows
    packed = rows * GROUPS
    f32, bf16 = jnp.float32, jnp.bfloat16
    vmem = pl.BlockSpec(memory_space=pltpu.VMEM)
    hbm = pl.BlockSpec(memory_space=pltpu.HBM)
    like = lambda array: pltpu.VMEM(array.shape, array.dtype)
    blocks = lambda: pltpu.VMEM((n_kv, packed, LANES), bf16)
    outs = (
        jax.ShapeDtypeStruct(residual_in.shape, residual_in.dtype),
        jax.ShapeDtypeStruct(memory_state.shape, memory_state.dtype),
    )
    layer, state = pl.pallas_call(
        functools.partial(fused_layer, n_kv),
        out_shape=tuple(pltpu.VMEM(out.shape, out.dtype) for out in outs),
        in_specs=[vmem] * 6 + [hbm] * 12,
        out_specs=(vmem, vmem),
        scratch_shapes=[
            pltpu.VMEM((hidden, width), bf16),
            pltpu.VMEM((hidden, width), bf16),
            like(down_pre),
            pltpu.VMEM((PLANE,) + query_weight.shape, bf16),
            pltpu.VMEM((PLANE,) + query_weight.shape, bf16),
            pltpu.VMEM((2, width, width), bf16),
            pltpu.VMEM((hidden, width), bf16),
            pltpu.VMEM((hidden, width), bf16),
            like(down_post),
            pltpu.VMEM((width, hidden), bf16),
            pltpu.VMEM((width, hidden), bf16),
            pltpu.VMEM((width, hidden), bf16),
            pltpu.VMEM((width, hidden), bf16),
            like(memory_state),
            pltpu.VMEM((rows // 2, width, 2 * LANES), bf16),
            blocks(),
            blocks(),
            pltpu.VMEM((n_kv * packed, LANES), f32),
            pltpu.VMEM((n_kv * packed, LANES), f32),
            pltpu.VMEM((n_kv * packed, LANES), f32),
            pltpu.VMEM((total, width), bf16),
            pltpu.VMEM((GROUPS, total, LANES), bf16),
            pltpu.VMEM((n_kv, total, LANES), bf16),
            pltpu.VMEM((PLANE, total, LANES), bf16),
            pltpu.VMEM((total, LANES), bf16),
            pltpu.VMEM((total, LANES), bf16),
            pltpu.VMEM((n_kv, rows, LANES), f32),
            pltpu.VMEM((GROUPS, rows, LANES), f32),
            pltpu.VMEM((packed, LANES), f32),
            blocks(),
            blocks(),
            pltpu.VMEM((packed, LANES), f32),
            pltpu.VMEM((rows, LANES, GROUPS), f32),
            pltpu.VMEM((rows, LANES, GROUPS), f32),
            pltpu.VMEM((packed, LANES), f32),
            pltpu.VMEM((GROUPS * GROUPS, LANES), f32),
            pltpu.VMEM((packed, LANES), f32),
            pltpu.VMEM((packed, LANES), f32),
            pltpu.VMEM((packed, LANES), f32),
            blocks(),
            blocks(),
            pltpu.VMEM((2, 2, total, hidden), bf16),
            pltpu.VMEM((2, 2, total, hidden), bf16),
            pltpu.VMEM((2, total, LANES), f32),
            pltpu.VMEM((2, total, LANES), f32),
            pltpu.VMEM((rows, LANES), f32),
            pltpu.VMEM((rows, LANES), f32),
            pltpu.SemaphoreType.DMA((13,)),
            pltpu.SemaphoreType.DMA((EXCHANGES,)),
            pltpu.SemaphoreType.DMA((EXCHANGES,)),
            pltpu.SemaphoreType.DMA((9,)),
            pltpu.SemaphoreType.DMA((9,)),
        ],
        compiler_params=pltpu.CompilerParams(
            collective_id=0, has_side_effects=True, vmem_limit_bytes=56 * 1024 * 1024
        ),
    )(
        residual_in,
        gain_pre.reshape(1, width),
        gain_mix.reshape(n_kv, 1, LANES),
        lower_bound.reshape(GROUPS, LANES),
        head_gain.reshape(GROUPS, LANES),
        gain_post.reshape(1, width),
        gate_pre.T,
        up_pre.T,
        down_pre,
        query_weight,
        forget_weight,
        value_weight,
        outgate_weight,
        out_weight,
        gate_post.T,
        up_post.T,
        down_post,
        memory_state,
    )
    return pl.pallas_call(
        store_results,
        out_shape=outs,
        in_specs=[vmem, vmem],
        out_specs=(hbm, hbm),
        scratch_shapes=[pltpu.SemaphoreType.DMA((1 + rows,))],
        compiler_params=pltpu.CompilerParams(vmem_limit_bytes=8 * 1024 * 1024),
    )(layer, state)


def solution(mesh):
    n_kv, n_tp = mesh.shape["kv"], mesh.shape["tp"]
    fits = n_tp == 2 and n_kv * LANES == D and n_kv // n_tp == GROUPS
    body = functools.partial(fused_shards, n_kv) if fits else shards
    in_specs = (
        P("kv", "tp"),
        P("tp"),
        P("tp", "kv"),
        P("tp", "kv"),
        P("kv", "tp"),
        P(),
        P("kv", "tp"),
        P("kv", "tp"),
        P("kv", "tp"),
        P("kv", "tp"),
        P("tp"),
        P("tp"),
        P("tp", None),
        P("tp"),
        P("tp", "kv"),
        P("tp", "kv"),
        P("kv", "tp"),
        P("kv", "tp", None, None),
    )
    out_specs = (P("kv", "tp"), P("kv", "tp", None, None))
    return jax.shard_map(body, mesh=mesh, in_specs=in_specs, out_specs=out_specs, check_vma=False)
```

```python
import functools

import jax
import jax.numpy as jnp
from jax import lax
from jax.experimental import pallas as pl
from jax.experimental.pallas import tpu as pltpu
from jax.sharding import PartitionSpec as P

D = 2048
HEAD_DIM = 128


EPSILON = 1e-06


def channel_mixer(row_block, gain_vec, gate_weight, up_weight, down_weight):
    gathered = lax.all_gather(row_block, "kv", axis=0, tiled=True)
    widened = gathered.astype(jnp.float32)
    part_squares = jnp.sum(widened * widened, axis=1)
    scaled = (widened * gain_vec).astype(jnp.bfloat16)
    gate_part = jnp.dot(scaled, gate_weight, preferred_element_type=jnp.float32)
    up_part = jnp.dot(scaled, up_weight, preferred_element_type=jnp.float32)
    gate_share, up_share, square_share = (
        lax.psum_scatter(
            gate_part.astype(jnp.bfloat16), "tp", scatter_dimension=0, tiled=True
        ).astype(jnp.float32),
        lax.psum_scatter(
            up_part.astype(jnp.bfloat16), "tp", scatter_dimension=0, tiled=True
        ).astype(jnp.float32),
        lax.psum_scatter(
            part_squares.astype(jnp.bfloat16), "tp", scatter_dimension=0, tiled=True
        ).astype(jnp.float32),
    )
    share_inverse = lax.rsqrt(square_share / D + EPSILON)[:, None]
    hidden_share = (jax.nn.silu(gate_share * share_inverse) * (up_share * share_inverse)).astype(
        jnp.bfloat16
    )
    hidden = lax.all_gather(hidden_share, "tp", axis=0, tiled=True)
    return lax.psum_scatter(
        jnp.dot(hidden, down_weight, preferred_element_type=jnp.float32),
        "kv",
        scatter_dimension=0,
        tiled=True,
    )


def token_mixer(
    stream_a,
    gain_mix,
    query_weight,
    forget_weight,
    value_weight,
    outgate_weight,
    lower_bound,
    head_gain,
    out_weight,
    memory_state,
):
    full_rows = lax.all_gather(stream_a, "tp", axis=1, tiled=True)
    widened = full_rows.astype(jnp.float32)
    inverse = lax.rsqrt(jnp.mean(widened * widened, axis=1, keepdims=True) + EPSILON)
    scaled = (widened * gain_mix).astype(jnp.bfloat16)
    weights = (query_weight, forget_weight, value_weight, outgate_weight)
    blocks = lax.all_to_all(scaled, "kv", split_axis=1, concat_axis=0, tiled=True)
    joined = jnp.concatenate(weights, axis=1)
    projected = lax.psum_scatter(
        jnp.dot(blocks, joined, preferred_element_type=jnp.float32),
        "kv",
        scatter_dimension=0,
        tiled=True,
    )
    projected = projected * inverse
    seq_rows = scaled.shape[0]
    local_heads = query_weight.shape[1] // HEAD_DIM
    reshaped = projected.reshape(seq_rows, 4, local_heads, HEAD_DIM)
    query_pre = reshaped[:, 0]
    forget_pre = reshaped[:, 1]
    value_pre = reshaped[:, 2]
    outgate_pre = reshaped[:, 3]
    floor_rate = lower_bound.reshape(local_heads, HEAD_DIM)
    log_keep = jnp.logaddexp(
        jnp.log(floor_rate), jnp.log1p(-floor_rate) + jax.nn.log_sigmoid(forget_pre)
    )
    inject = (1.0 - floor_rate) * jax.nn.sigmoid(-forget_pre)
    next_state = (
        jnp.exp(log_keep)[..., None] * memory_state + inject[..., None] * value_pre[:, :, None, :]
    )
    readout = jnp.einsum(
        "bhk,bhkv->bhv", jax.nn.silu(query_pre), next_state, precision=lax.Precision.HIGHEST
    )
    normed = (
        readout
        * lax.rsqrt(jnp.mean(readout * readout, axis=2, keepdims=True) + EPSILON)
        * head_gain.reshape(local_heads, HEAD_DIM)
    )
    mixed_heads = (
        (normed * jax.nn.silu(outgate_pre))
        .reshape(seq_rows, local_heads * HEAD_DIM)
        .astype(jnp.bfloat16)
    )
    partial_out = jnp.dot(mixed_heads, out_weight, preferred_element_type=jnp.float32)
    mixed = lax.psum_scatter(
        partial_out.astype(jnp.bfloat16), "tp", scatter_dimension=1, tiled=True
    ).astype(jnp.float32)
    return (mixed, next_state)


def shards(
    residual_in,
    gain_pre,
    gate_pre,
    up_pre,
    down_pre,
    gain_mix,
    query_weight,
    forget_weight,
    value_weight,
    outgate_weight,
    lower_bound,
    head_gain,
    out_weight,
    gain_post,
    gate_post,
    up_post,
    down_post,
    memory_state,
):
    branch_a = channel_mixer(residual_in, gain_pre, gate_pre, up_pre, down_pre)
    stream_a = (residual_in.astype(jnp.float32) + 0.5 * branch_a).astype(jnp.bfloat16)
    mixed, next_state = token_mixer(
        stream_a,
        gain_mix,
        query_weight,
        forget_weight,
        value_weight,
        outgate_weight,
        lower_bound,
        head_gain,
        out_weight,
        memory_state,
    )
    stream_b = (stream_a.astype(jnp.float32) + mixed).astype(jnp.bfloat16)
    branch_b = channel_mixer(stream_b, gain_post, gate_post, up_post, down_post)
    layer_out = (stream_b.astype(jnp.float32) + 0.5 * branch_b).astype(jnp.bfloat16)
    return (layer_out, next_state)


LANES = 128
GROUPS = 8
PLANE = 4
HALVES = 2
GATHER_A, SCATTER_A, SHARE, PROJECT, GATHER_B, SCATTER_B, WEIGHTS, ROWS = range(0, 16, HALVES)
EXCHANGES = 16
SQUARES, MIXED, COLUMNS = 12, 13, 14
TP_EXCHANGES = 16
HOLDER = 1
WEIGHTS_EARLY = ((1, 0, 128), (2, 0, 128))
WEIGHTS_MIDDLE = ((3, 0, 32),)
WEIGHTS_LATE = ((3, 32, 128),)
FLIPS = (3, 1, 2, 0)


def lanes(group):
    return slice(group * LANES, (group + 1) * LANES)


def fused_layer(
    n_kv,
    residual_ref,
    gain_pre_ref,
    gain_mix_ref,
    lower_ref,
    head_gain_ref,
    gain_post_ref,
    gate_pre_hbm,
    up_pre_hbm,
    down_pre_hbm,
    query_hbm,
    forget_hbm,
    value_hbm,
    outgate_hbm,
    out_hbm,
    gate_post_hbm,
    up_post_hbm,
    down_post_hbm,
    state_hbm,
    layer_ref,
    next_ref,
    gate_pre,
    up_pre,
    down_pre,
    own_weights,
    plane_weights,
    out_weight,
    gate_post,
    up_post,
    down_post,
    gate_pre_t,
    up_pre_t,
    gate_post_t,
    up_post_t,
    state,
    state_half,
    gather_a,
    gather_b,
    wide_a,
    wide_b,
    spread,
    scaled_rows,
    columns_out,
    columns_landed,
    columns_in,
    shared_out,
    shared_in,
    rows_out,
    rows_in,
    stream_rows,
    proj_out,
    proj_in,
    inverse_rows,
    keep_t,
    inject_t,
    value_rows,
    mixed_rows,
    mixed_out,
    mixed_own,
    mixed_in,
    partial_b,
    landed_b,
    gate_up_out,
    gate_up_in,
    squares_out,
    squares_in,
    row_squares_out,
    row_squares_in,
    load_sem,
    send_sem,
    recv_sem,
    tp_send,
    tp_recv,
):
    me = lax.axis_index("kv")
    core = lax.axis_index("tp")
    rows, width = residual_ref.shape
    model = 2 * width
    total = n_kv * rows
    packed = rows * GROUPS
    part = rows // HALVES
    part_total = n_kv * part
    part_packed = part * GROUPS
    planes = n_kv // PLANE
    half_planes = planes // 2
    depth_at, spot = me // PLANE, lax.rem(me, PLANE)
    spot_x, spot_y = lax.rem(spot, 2), spot // 2
    slot = lax.rem(me, GROUPS)
    owner_core = me // GROUPS
    holder = core == HOLDER
    owns = jnp.logical_and(holder, owner_core == HOLDER)
    f32, bf16 = jnp.float32, jnp.bfloat16

    def flipped(flip):
        return 2 * lax.rem(spot_y + flip // 2, 2) + lax.rem(spot_x + flip % 2, 2)

    def others():
        for flip in FLIPS:
            for step in range(planes - 1, -1, -1):
                plane = 2 * lax.rem(depth_at // 2 + step // 2, 2) + lax.rem(depth_at + step, 2)
                if step or flip:
                    yield plane * PLANE + flipped(flip)

    def load(index, source, target):
        return pltpu.make_async_copy(source, target, load_sem.at[index])

    loads = [
        load(0, forget_hbm, own_weights.at[0]),
        load(1, value_hbm, own_weights.at[1]),
        load(2, query_hbm, own_weights.at[2]),
        load(3, outgate_hbm, own_weights.at[3]),
        load(4, gate_pre_hbm, gate_pre),
        load(5, up_pre_hbm, up_pre),
        load(6, down_pre_hbm, down_pre),
        load(7, state_hbm, state),
        load(8, out_hbm.at[:, pl.ds(0, width)], out_weight.at[0]),
        load(12, out_hbm.at[:, pl.ds(width, width)], out_weight.at[1]),
        load(9, gate_post_hbm, gate_post),
        load(10, up_post_hbm, up_post),
        load(11, down_post_hbm, down_post),
    ]
    for copy in loads:
        copy.start()

    def spread_rows(target, values):
        for group in range(GROUPS):
            target[pl.ds(group, values.shape[0], stride=GROUPS), :] = values[:, lanes(group)]

    residual = residual_ref[...].astype(f32)
    spread_rows(stream_rows, residual)
    packed_parts = [
        slice(half * part_packed, (half + 1) * part_packed) for half in range(HALVES)
    ]
    for half in range(HALVES):
        gather_a[half, me] = stream_rows[packed_parts[half], :].astype(bf16)

    barrier = pltpu.get_barrier_semaphore()
    for peer in others():
        pl.semaphore_signal(
            barrier, inc=1, device_id={"kv": peer}, device_id_type=pl.DeviceIdType.MESH
        )
    pl.semaphore_signal(
        barrier, inc=1, device_id={"tp": 1 - core}, device_id_type=pl.DeviceIdType.MESH
    )
    pl.semaphore_wait(barrier, n_kv)

    def remote(exchange, source, target, **device):
        return pltpu.make_async_remote_copy(
            src_ref=source,
            dst_ref=target,
            send_sem=send_sem.at[exchange],
            recv_sem=recv_sem.at[exchange],
            device_id=device,
            device_id_type=pl.DeviceIdType.MESH,
        )

    def all_of(exchange, ref):
        return remote(exchange, ref, ref, tp=1 - core)

    def tp_copy(index, source, target):
        return pltpu.make_async_remote_copy(
            src_ref=source,
            dst_ref=target,
            send_sem=tp_send.at[index],
            recv_sem=tp_recv.at[index],
            device_id={"tp": 1 - core},
            device_id_type=pl.DeviceIdType.MESH,
        )

    def gate_up(which, half, gathered, wide, gain_ref, gate, up):
        wide[half] = gathered[half].astype(f32).reshape(part_total * GROUPS, LANES)
        square_lanes = jnp.zeros((part_total, LANES), f32)
        for group in range(GROUPS):
            piece = wide[half, pl.ds(group, part_total, stride=GROUPS), :]
            square_lanes += piece * piece
            scaled_rows[half, :, lanes(group)] = (piece * gain_ref[:, lanes(group)]).astype(bf16)
        scaled = scaled_rows[half]
        squares = jnp.sum(square_lanes, axis=1, keepdims=True)
        squares_out[which, half] = jnp.broadcast_to(squares, squares_out.shape[2:])
        first = 6 * which + 3 * half
        copies = [
            tp_copy(first, squares_out.at[which, half], squares_in.at[which, half]),
            tp_copy(first + 1, gate_up_out.at[which, half, 0], gate_up_in.at[which, half, 0]),
            tp_copy(first + 2, gate_up_out.at[which, half, 1], gate_up_in.at[which, half, 1]),
        ]
        gate_part = jnp.dot(scaled, gate[...], preferred_element_type=f32)
        gate_up_out[which, half, 0] = gate_part.astype(bf16)
        copies[0].start()
        copies[1].start()
        up_part = jnp.dot(scaled, up[...], preferred_element_type=f32)
        gate_up_out[which, half, 1] = up_part.astype(bf16)
        copies[2].start()
        return squares, gate_part, up_part, copies

    def down_sum(which, half, parts, down):
        squares, gate_part, up_part, copies = parts
        for copy in copies:
            copy.wait_recv()
        inverse = lax.rsqrt((squares + squares_in[which, half][:, 0:1]) / model + EPSILON)
        gate_sum = (gate_part + gate_up_in[which, half, 0].astype(f32)) * inverse
        up_sum = (up_part + gate_up_in[which, half, 1].astype(f32)) * inverse
        hidden = (gate_sum / (1.0 + jnp.exp(-gate_sum)) * up_sum).astype(bf16)
        return jnp.dot(hidden, down[...], preferred_element_type=f32)

    def gather_start(exchange, gathered):
        for half in range(HALVES):
            block = gathered.at[half, me]
            for peer in others():
                remote(exchange + half, block, block, kv=peer).start()

    def turn(target, source):
        for group in range(GROUPS):
            target[lanes(group), :] = source[:, lanes(group)].T

    def but_one(ref, half):
        return ref.at[half, pl.ds(0, n_kv - 1)]

    gather_start(GATHER_A, gather_a)
    for copy in loads[0:4]:
        copy.wait()
    def send_weights(*flips):
        for flip, low, high in flips:
            peer_spot = flipped(flip)
            span = pl.ds(low, high - low)
            remote(
                WEIGHTS,
                own_weights.at[peer_spot, span],
                plane_weights.at[spot, span],
                kv=depth_at * PLANE + peer_spot,
            ).start()

    send_weights(*WEIGHTS_EARLY)
    plane_weights[spot] = own_weights[spot]
    mixed_rows[packed:, :] = jnp.zeros((mixed_rows.shape[0] - packed, LANES), f32)
    for copy in loads[4:7]:
        copy.wait()
    turn(gate_pre_t, gate_pre)
    turn(up_pre_t, up_pre)
    parts_a = []
    for half in range(HALVES):
        all_of(GATHER_A + half, but_one(gather_a, half)).wait_recv()
        if half == HALVES - 1:
            send_weights(*WEIGHTS_MIDDLE)
        parts_a.append(
            gate_up(0, half, gather_a, wide_a, gain_pre_ref, gate_pre_t, up_pre_t)
        )
    shared_copies = [
        tp_copy(COLUMNS + half, shared_out.at[half], shared_in.at[half]) for half in range(HALVES)
    ]

    @pl.when(owner_core == core)
    def _():
        for half in range(HALVES):
            shared_out[half] = wide_a[half, pl.ds(slot, part_total, stride=GROUPS), :].astype(bf16)

        @pl.when(jnp.logical_not(holder))
        def _():
            for copy in shared_copies:
                copy.start()

    for half in range(HALVES):
        branch_a = down_sum(0, half, parts_a[half], down_pre)
        for group in range(GROUPS):
            columns_out[half, group] = branch_a[:, lanes(group)].astype(bf16)
        for flip in FLIPS:
            for step in range(half_planes - 1, -1, -1):
                plane = core * half_planes + lax.rem(depth_at + step, half_planes)
                peer = plane * PLANE + flipped(flip)
                copy = remote(
                    SCATTER_A + half,
                    columns_out.at[half, lax.rem(peer, GROUPS)],
                    columns_landed.at[half, me],
                    kv=peer,
                    tp=HOLDER,
                )
                if step or flip:
                    copy.start()
                else:
                    pl.when(jnp.logical_not(owns))(copy.start)

    send_weights(*WEIGHTS_LATE)

    @pl.when(holder)
    def _():
        for half in range(HALVES):

            @pl.when(owns)
            def _():
                columns_landed[half, me] = columns_out[half, slot]
                shared_in[half] = shared_out[half]
                all_of(SCATTER_A + half, but_one(columns_landed, half)).wait_recv()

            @pl.when(jnp.logical_not(owns))
            def _():
                shared_copies[half].wait_recv()
                all_of(SCATTER_A + half, columns_landed.at[half]).wait_recv()

            branch = jnp.sum(columns_landed[half].astype(f32), axis=0)
            stream = (shared_in[half].astype(f32) + 0.5 * branch).astype(bf16).astype(f32)
            columns_in[half, spot] = (stream * gain_mix_ref[me]).astype(bf16)
            block = columns_in.at[half, spot]
            for flip in FLIPS:
                peer = depth_at * PLANE + flipped(flip)
                remote(SHARE + half, block, block, kv=peer, tp=1 - core).start()
                if flip:
                    remote(SHARE + half, block, block, kv=peer, tp=core).start()
            for owner in range(n_kv):
                rows_out[owner, half * part : (half + 1) * part, :] = stream[
                    owner * part : (owner + 1) * part, :
                ]
        for peer in others():
            remote(ROWS, rows_out.at[peer], rows_in.at[slot], kv=peer, tp=owner_core).start()

        @pl.when(owns)
        def _():
            rows_in[slot] = rows_out[me]

        @pl.when(jnp.logical_not(owns))
        def _():
            remote(ROWS, rows_out.at[me], rows_in.at[slot], tp=1 - core).start()

    for half in range(HALVES):

        @pl.when(holder)
        def _():
            all_of(SHARE + half, columns_in.at[half, pl.ds(0, PLANE - 1)]).wait_recv()

        @pl.when(jnp.logical_not(holder))
        def _():
            all_of(SHARE + half, columns_in.at[half]).wait_recv()

        if half == 0:
            all_of(WEIGHTS, plane_weights.at[pl.ds(0, PLANE - 1)]).wait_recv()
        columns = jnp.concatenate([columns_in[half, place] for place in range(PLANE)], axis=1)
        product = jnp.dot(
            columns,
            plane_weights[...].reshape(PLANE * LANES, width),
            preferred_element_type=f32,
        )
        spread_rows(spread.at[half], product)
        proj_out[half] = spread[half].astype(bf16).reshape(n_kv, part_packed, LANES)
        for peer in others():
            remote(PROJECT + half, proj_out.at[half, peer], proj_in.at[half, me], kv=peer).start()
        proj_in[half, me] = proj_out[half, me]

    @pl.when(owns)
    def _():
        all_of(ROWS, rows_in.at[pl.ds(0, GROUPS - 1)]).wait_recv()

    @pl.when(jnp.logical_not(owns))
    def _():
        all_of(ROWS, rows_in).wait_recv()

    for group in range(GROUPS):
        stream_rows[pl.ds(group, rows, stride=GROUPS), :] = rows_in[group]
    stream = stream_rows[...].reshape(rows, GROUPS, LANES)
    row_squares = jnp.sum(stream * stream, axis=1)
    row_squares_out[...] = row_squares
    square_copy = tp_copy(SQUARES, row_squares_out, row_squares_in)
    square_copy.start()
    loads[7].wait()
    for row in range(rows):
        for head in range(GROUPS):
            state_half[row // 2, head * LANES : (head + 1) * LANES, lanes(row % 2)] = state[
                row, head
            ].astype(bf16)
    for copy in loads[10:12]:
        copy.wait()
    turn(gate_post_t, gate_post)
    turn(up_post_t, up_post)
    square_copy.wait_recv()
    squares = jnp.sum(row_squares + row_squares_in[...], axis=1, keepdims=True)
    inverse = lax.rsqrt(squares / model + EPSILON)
    for row in range(rows):
        inverse_rows[row * GROUPS : (row + 1) * GROUPS, :] = jnp.broadcast_to(
            inverse[row : row + 1, :], (GROUPS, LANES)
        )
    loads[8].wait()
    loads[9].wait()
    for half in range(HALVES):
        all_of(PROJECT + half, but_one(proj_in, half)).wait_recv()

    def projected(index):
        sums = []
        for half in range(HALVES):
            terms = [proj_in[half, plane * PLANE + index].astype(f32) for plane in range(planes)]
            sums.append(sum(terms[1:], terms[0]))
        return jnp.concatenate(sums, axis=0) * inverse_rows[...]

    floor_rate = jnp.concatenate([lower_ref[...]] * rows, axis=0)
    forget_pre = projected(0)
    keep = floor_rate + (1.0 - floor_rate) / (1.0 + jnp.exp(-forget_pre))
    inject = (1.0 - floor_rate) / (1.0 + jnp.exp(forget_pre))
    query_pre = projected(2)
    query = query_pre / (1.0 + jnp.exp(-query_pre))
    value = projected(1)
    value_rows[...] = value
    weighted = query * keep
    direct = jnp.sum(query * inject, axis=1, keepdims=True) * value
    head_index = lax.broadcasted_iota(jnp.int32, (GROUPS, LANES), 0)
    read = []
    for pair in range(rows // 2):
        diagonal = []
        for row in (2 * pair, 2 * pair + 1):
            heads = weighted[row * GROUPS : (row + 1) * GROUPS, :]
            diagonal.append(
                jnp.concatenate(
                    [jnp.where(head_index == head, heads, 0.0) for head in range(GROUPS)], axis=1
                )
            )
        both = jnp.dot(
            jnp.concatenate(diagonal, axis=0).astype(bf16),
            state_half[pair],
            preferred_element_type=f32,
        )
        read.append(both[0:GROUPS, lanes(0)])
        read.append(both[GROUPS : 2 * GROUPS, lanes(1)])
    readout = jnp.concatenate(read, axis=0) + direct
    outgate_pre = projected(3)
    outgate = outgate_pre / (1.0 + jnp.exp(-outgate_pre))
    scale = lax.rsqrt(jnp.mean(readout * readout, axis=1, keepdims=True) + EPSILON)
    head_gain = jnp.concatenate([head_gain_ref[...]] * rows, axis=0)
    mixed_rows[0:packed, :] = readout * scale * head_gain * outgate
    mixed_heads = jnp.concatenate(
        [mixed_rows[pl.ds(head, GROUPS, stride=GROUPS), :] for head in range(GROUPS)], axis=1
    ).astype(bf16)
    away = jnp.dot(mixed_heads, out_weight[1 - core], preferred_element_type=f32)
    spread_rows(mixed_out, away[0:rows])
    mixed_copy = tp_copy(MIXED, mixed_out, mixed_in)
    mixed_copy.start()
    home = jnp.dot(mixed_heads, out_weight[core], preferred_element_type=f32)
    spread_rows(mixed_own, home[0:rows])
    for row in range(rows):
        span = slice(row * GROUPS, (row + 1) * GROUPS)
        keep_t[row] = keep[span].T
        inject_t[row] = inject[span].T
    mixed_copy.wait_recv()
    stream_b = (stream_rows[...] + (mixed_own[...] + mixed_in[...])).astype(bf16)
    for half in range(HALVES):
        gather_b[half, me] = stream_b[packed_parts[half], :]
    gather_start(GATHER_B, gather_b)

    def update(row, carry):
        keep_columns = keep_t[row]
        inject_columns = inject_t[row]
        for head in range(GROUPS):
            column = slice(head, head + 1)
            values = value_rows[pl.ds(row * GROUPS + head, 1), :]
            next_ref[row, head] = (
                keep_columns[:, column] * state[row, head] + inject_columns[:, column] * values
            )
        return carry

    lax.fori_loop(0, rows, update, 0)
    loads[12].wait()
    parts_b = []
    for half in range(HALVES):
        all_of(GATHER_B + half, but_one(gather_b, half)).wait_recv()
        parts_b.append(
            gate_up(1, half, gather_b, wide_b, gain_post_ref, gate_post_t, up_post_t)
        )
    for half in range(HALVES):
        branch_b = down_sum(1, half, parts_b[half], down_post)
        spread_rows(spread.at[half], branch_b)
        partial_b[half] = spread[half].astype(bf16).reshape(n_kv, part_packed, LANES)
        for peer in others():
            remote(
                SCATTER_B + half, partial_b.at[half, peer], landed_b.at[half, me], kv=peer
            ).start()
        landed_b[half, me] = partial_b[half, me]
    for copy in parts_a[0][3] + parts_a[1][3] + parts_b[0][3] + parts_b[1][3]:
        copy.wait_send()
    square_copy.wait_send()
    mixed_copy.wait_send()
    all_of(WEIGHTS, plane_weights.at[pl.ds(0, PLANE - 1)]).wait_send()
    for half in range(HALVES):
        all_of(GATHER_A + half, but_one(gather_a, half)).wait_send()
        all_of(PROJECT + half, but_one(proj_out, half)).wait_send()
        all_of(GATHER_B + half, but_one(gather_b, half)).wait_send()

    @pl.when(holder)
    def _():
        for half in range(HALVES):
            all_of(SHARE + half, columns_landed.at[half, pl.ds(0, 2 * PLANE - 1)]).wait_send()

    @pl.when(owns)
    def _():
        for half in range(HALVES):
            all_of(SCATTER_A + half, columns_out.at[half, pl.ds(0, GROUPS - 1)]).wait_send()
        all_of(ROWS, rows_out.at[pl.ds(0, n_kv - 1)]).wait_send()

    @pl.when(jnp.logical_not(owns))
    def _():
        for half in range(HALVES):
            all_of(SCATTER_A + half, columns_out.at[half]).wait_send()

        @pl.when(holder)
        def _():
            all_of(ROWS, rows_out).wait_send()

    @pl.when(jnp.logical_and(owner_core == core, jnp.logical_not(holder)))
    def _():
        for copy in shared_copies:
            copy.wait_send()

    for half in range(HALVES):
        all_of(SCATTER_B + half, but_one(landed_b, half)).wait_recv()
        branch = jnp.sum(landed_b[half].astype(f32), axis=0)
        mixed_rows[packed_parts[half], :] = gather_b[half, me].astype(f32) + 0.5 * branch
    for group in range(GROUPS):
        layer_ref[:, lanes(group)] = mixed_rows[pl.ds(group, rows, stride=GROUPS), :].astype(bf16)
    for half in range(HALVES):
        all_of(SCATTER_B + half, but_one(partial_b, half)).wait_send()


def store_results(layer_in, state_in, layer_out, state_out, sem):
    copies = [pltpu.make_async_copy(layer_in, layer_out, sem.at[0])]
    for row in range(state_in.shape[0]):
        copies.append(pltpu.make_async_copy(state_in.at[row], state_out.at[row], sem.at[1 + row]))
    for copy in copies:
        copy.start()
    for copy in copies:
        copy.wait()


def fused_shards(
    n_kv,
    residual_in,
    gain_pre,
    gate_pre,
    up_pre,
    down_pre,
    gain_mix,
    query_weight,
    forget_weight,
    value_weight,
    outgate_weight,
    lower_bound,
    head_gain,
    out_weight,
    gain_post,
    gate_post,
    up_post,
    down_post,
    memory_state,
):
    rows, width = residual_in.shape
    hidden = gate_pre.shape[1]
    total = n_kv * rows
    packed = rows * GROUPS
    f32, bf16 = jnp.float32, jnp.bfloat16
    vmem = pl.BlockSpec(memory_space=pltpu.VMEM)
    hbm = pl.BlockSpec(memory_space=pltpu.HBM)
    like = lambda array: pltpu.VMEM(array.shape, array.dtype)
    part_total = total // HALVES
    blocks = lambda: pltpu.VMEM((HALVES, n_kv, packed // HALVES, LANES), bf16)
    halves = lambda *shape: pltpu.VMEM((HALVES,) + shape, bf16)
    outs = (
        jax.ShapeDtypeStruct(residual_in.shape, residual_in.dtype),
        jax.ShapeDtypeStruct(memory_state.shape, memory_state.dtype),
    )
    layer, state = pl.pallas_call(
        functools.partial(fused_layer, n_kv),
        out_shape=tuple(pltpu.VMEM(out.shape, out.dtype) for out in outs),
        in_specs=[vmem] * 6 + [hbm] * 12,
        out_specs=(vmem, vmem),
        scratch_shapes=[
            pltpu.VMEM((hidden, width), bf16),
            pltpu.VMEM((hidden, width), bf16),
            like(down_pre),
            pltpu.VMEM((PLANE,) + query_weight.shape, bf16),
            pltpu.VMEM((PLANE,) + query_weight.shape, bf16),
            pltpu.VMEM((2, width, width), bf16),
            pltpu.VMEM((hidden, width), bf16),
            pltpu.VMEM((hidden, width), bf16),
            like(down_post),
            pltpu.VMEM((width, hidden), bf16),
            pltpu.VMEM((width, hidden), bf16),
            pltpu.VMEM((width, hidden), bf16),
            pltpu.VMEM((width, hidden), bf16),
            like(memory_state),
            pltpu.VMEM((rows // 2, width, 2 * LANES), bf16),
            blocks(),
            blocks(),
            pltpu.VMEM((HALVES, part_total * GROUPS, LANES), f32),
            pltpu.VMEM((HALVES, part_total * GROUPS, LANES), f32),
            pltpu.VMEM((HALVES, part_total * GROUPS, LANES), f32),
            halves(part_total, width),
            halves(GROUPS, part_total, LANES),
            halves(n_kv, part_total, LANES),
            halves(PLANE, part_total, LANES),
            halves(part_total, LANES),
            halves(part_total, LANES),
            pltpu.VMEM((n_kv, rows, LANES), f32),
            pltpu.VMEM((GROUPS, rows, LANES), f32),
            pltpu.VMEM((packed, LANES), f32),
            blocks(),
            blocks(),
            pltpu.VMEM((packed, LANES), f32),
            pltpu.VMEM((rows, LANES, GROUPS), f32),
            pltpu.VMEM((rows, LANES, GROUPS), f32),
            pltpu.VMEM((packed, LANES), f32),
            pltpu.VMEM((GROUPS * GROUPS, LANES), f32),
            pltpu.VMEM((packed, LANES), f32),
            pltpu.VMEM((packed, LANES), f32),
            pltpu.VMEM((packed, LANES), f32),
            blocks(),
            blocks(),
            pltpu.VMEM((2, HALVES, 2, part_total, hidden), bf16),
            pltpu.VMEM((2, HALVES, 2, part_total, hidden), bf16),
            pltpu.VMEM((2, HALVES, part_total, LANES), f32),
            pltpu.VMEM((2, HALVES, part_total, LANES), f32),
            pltpu.VMEM((rows, LANES), f32),
            pltpu.VMEM((rows, LANES), f32),
            pltpu.SemaphoreType.DMA((13,)),
            pltpu.SemaphoreType.DMA((EXCHANGES,)),
            pltpu.SemaphoreType.DMA((EXCHANGES,)),
            pltpu.SemaphoreType.DMA((TP_EXCHANGES,)),
            pltpu.SemaphoreType.DMA((TP_EXCHANGES,)),
        ],
        compiler_params=pltpu.CompilerParams(
            collective_id=0, has_side_effects=True, vmem_limit_bytes=56 * 1024 * 1024
        ),
    )(
        residual_in,
        gain_pre.reshape(1, width),
        gain_mix.reshape(n_kv, 1, LANES),
        lower_bound.reshape(GROUPS, LANES),
        head_gain.reshape(GROUPS, LANES),
        gain_post.reshape(1, width),
        gate_pre.T,
        up_pre.T,
        down_pre,
        query_weight,
        forget_weight,
        value_weight,
        outgate_weight,
        out_weight,
        gate_post.T,
        up_post.T,
        down_post,
        memory_state,
    )
    return pl.pallas_call(
        store_results,
        out_shape=outs,
        in_specs=[vmem, vmem],
        out_specs=(hbm, hbm),
        scratch_shapes=[pltpu.SemaphoreType.DMA((1 + rows,))],
        compiler_params=pltpu.CompilerParams(vmem_limit_bytes=8 * 1024 * 1024),
    )(layer, state)


def solution(mesh):
    n_kv, n_tp = mesh.shape["kv"], mesh.shape["tp"]
    fits = n_tp == 2 and n_kv * LANES == D and n_kv // n_tp == GROUPS
    body = functools.partial(fused_shards, n_kv) if fits else shards
    in_specs = (
        P("kv", "tp"),
        P("tp"),
        P("tp", "kv"),
        P("tp", "kv"),
        P("kv", "tp"),
        P(),
        P("kv", "tp"),
        P("kv", "tp"),
        P("kv", "tp"),
        P("kv", "tp"),
        P("tp"),
        P("tp"),
        P("tp", None),
        P("tp"),
        P("tp", "kv"),
        P("tp", "kv"),
        P("kv", "tp"),
        P("kv", "tp", None, None),
    )
    out_specs = (P("kv", "tp"), P("kv", "tp", None, None))
    return jax.shard_map(body, mesh=mesh, in_specs=in_specs, out_specs=out_specs, check_vma=False)
```

```python
import functools

import jax
import jax.numpy as jnp
from jax import lax
from jax.experimental import pallas as pl
from jax.experimental.pallas import tpu as pltpu
from jax.sharding import PartitionSpec as P

D = 2048
HEAD_DIM = 128


EPSILON = 1e-06


def channel_mixer(row_block, gain_vec, gate_weight, up_weight, down_weight):
    gathered = lax.all_gather(row_block, "kv", axis=0, tiled=True)
    widened = gathered.astype(jnp.float32)
    part_squares = jnp.sum(widened * widened, axis=1)
    scaled = (widened * gain_vec).astype(jnp.bfloat16)
    gate_part = jnp.dot(scaled, gate_weight, preferred_element_type=jnp.float32)
    up_part = jnp.dot(scaled, up_weight, preferred_element_type=jnp.float32)
    gate_share, up_share, square_share = (
        lax.psum_scatter(
            gate_part.astype(jnp.bfloat16), "tp", scatter_dimension=0, tiled=True
        ).astype(jnp.float32),
        lax.psum_scatter(
            up_part.astype(jnp.bfloat16), "tp", scatter_dimension=0, tiled=True
        ).astype(jnp.float32),
        lax.psum_scatter(
            part_squares.astype(jnp.bfloat16), "tp", scatter_dimension=0, tiled=True
        ).astype(jnp.float32),
    )
    share_inverse = lax.rsqrt(square_share / D + EPSILON)[:, None]
    hidden_share = (jax.nn.silu(gate_share * share_inverse) * (up_share * share_inverse)).astype(
        jnp.bfloat16
    )
    hidden = lax.all_gather(hidden_share, "tp", axis=0, tiled=True)
    return lax.psum_scatter(
        jnp.dot(hidden, down_weight, preferred_element_type=jnp.float32),
        "kv",
        scatter_dimension=0,
        tiled=True,
    )


def token_mixer(
    stream_a,
    gain_mix,
    query_weight,
    forget_weight,
    value_weight,
    outgate_weight,
    lower_bound,
    head_gain,
    out_weight,
    memory_state,
):
    full_rows = lax.all_gather(stream_a, "tp", axis=1, tiled=True)
    widened = full_rows.astype(jnp.float32)
    inverse = lax.rsqrt(jnp.mean(widened * widened, axis=1, keepdims=True) + EPSILON)
    scaled = (widened * gain_mix).astype(jnp.bfloat16)
    weights = (query_weight, forget_weight, value_weight, outgate_weight)
    blocks = lax.all_to_all(scaled, "kv", split_axis=1, concat_axis=0, tiled=True)
    joined = jnp.concatenate(weights, axis=1)
    projected = lax.psum_scatter(
        jnp.dot(blocks, joined, preferred_element_type=jnp.float32),
        "kv",
        scatter_dimension=0,
        tiled=True,
    )
    projected = projected * inverse
    seq_rows = scaled.shape[0]
    local_heads = query_weight.shape[1] // HEAD_DIM
    reshaped = projected.reshape(seq_rows, 4, local_heads, HEAD_DIM)
    query_pre = reshaped[:, 0]
    forget_pre = reshaped[:, 1]
    value_pre = reshaped[:, 2]
    outgate_pre = reshaped[:, 3]
    floor_rate = lower_bound.reshape(local_heads, HEAD_DIM)
    log_keep = jnp.logaddexp(
        jnp.log(floor_rate), jnp.log1p(-floor_rate) + jax.nn.log_sigmoid(forget_pre)
    )
    inject = (1.0 - floor_rate) * jax.nn.sigmoid(-forget_pre)
    next_state = (
        jnp.exp(log_keep)[..., None] * memory_state + inject[..., None] * value_pre[:, :, None, :]
    )
    readout = jnp.einsum(
        "bhk,bhkv->bhv", jax.nn.silu(query_pre), next_state, precision=lax.Precision.HIGHEST
    )
    normed = (
        readout
        * lax.rsqrt(jnp.mean(readout * readout, axis=2, keepdims=True) + EPSILON)
        * head_gain.reshape(local_heads, HEAD_DIM)
    )
    mixed_heads = (
        (normed * jax.nn.silu(outgate_pre))
        .reshape(seq_rows, local_heads * HEAD_DIM)
        .astype(jnp.bfloat16)
    )
    partial_out = jnp.dot(mixed_heads, out_weight, preferred_element_type=jnp.float32)
    mixed = lax.psum_scatter(
        partial_out.astype(jnp.bfloat16), "tp", scatter_dimension=1, tiled=True
    ).astype(jnp.float32)
    return (mixed, next_state)


def shards(
    residual_in,
    gain_pre,
    gate_pre,
    up_pre,
    down_pre,
    gain_mix,
    query_weight,
    forget_weight,
    value_weight,
    outgate_weight,
    lower_bound,
    head_gain,
    out_weight,
    gain_post,
    gate_post,
    up_post,
    down_post,
    memory_state,
):
    branch_a = channel_mixer(residual_in, gain_pre, gate_pre, up_pre, down_pre)
    stream_a = (residual_in.astype(jnp.float32) + 0.5 * branch_a).astype(jnp.bfloat16)
    mixed, next_state = token_mixer(
        stream_a,
        gain_mix,
        query_weight,
        forget_weight,
        value_weight,
        outgate_weight,
        lower_bound,
        head_gain,
        out_weight,
        memory_state,
    )
    stream_b = (stream_a.astype(jnp.float32) + mixed).astype(jnp.bfloat16)
    branch_b = channel_mixer(stream_b, gain_post, gate_post, up_post, down_post)
    layer_out = (stream_b.astype(jnp.float32) + 0.5 * branch_b).astype(jnp.bfloat16)
    return (layer_out, next_state)


LANES = 128
GROUPS = 8
PLANE = 4
HALVES = 2
GATHER_A, SCATTER_A, SHARE, PROJECT, GATHER_B, SCATTER_B, WEIGHTS, ROWS = range(0, 16, HALVES)
EXCHANGES = 17
RELAY = 16
SQUARES, MIXED, COLUMNS = 12, 13, 14
TP_EXCHANGES = 16
HOLDER = 1
EARLY_ROWS = LANES // 4
WEIGHTS_EARLY = ((3, 0, LANES), (1, 0, EARLY_ROWS), (2, 0, EARLY_ROWS))
WEIGHTS_LATE = ((1, EARLY_ROWS, LANES), (2, EARLY_ROWS, LANES))
FLIPS = (3, 1, 2, 0)


def lanes(group):
    return slice(group * LANES, (group + 1) * LANES)


def fused_layer(
    n_kv,
    residual_ref,
    gain_pre_ref,
    gain_mix_ref,
    lower_ref,
    head_gain_ref,
    gain_post_ref,
    gate_pre_hbm,
    up_pre_hbm,
    down_pre_hbm,
    query_hbm,
    forget_hbm,
    value_hbm,
    outgate_hbm,
    out_hbm,
    gate_post_hbm,
    up_post_hbm,
    down_post_hbm,
    state_hbm,
    layer_ref,
    next_ref,
    gate_pre,
    up_pre,
    down_pre,
    own_weights,
    plane_weights,
    relayed,
    out_weight,
    gate_post,
    up_post,
    down_post,
    gate_pre_t,
    up_pre_t,
    gate_post_t,
    up_post_t,
    state,
    state_half,
    gather_a,
    gather_b,
    wide_a,
    wide_b,
    spread,
    scaled_rows,
    columns_out,
    columns_landed,
    columns_in,
    shared_out,
    shared_in,
    rows_out,
    rows_in,
    stream_rows,
    proj_out,
    proj_in,
    inverse_rows,
    keep_t,
    inject_t,
    value_rows,
    mixed_rows,
    mixed_out,
    mixed_own,
    mixed_in,
    partial_b,
    landed_b,
    gate_up_out,
    gate_up_in,
    squares_out,
    squares_in,
    row_squares_out,
    row_squares_in,
    load_sem,
    send_sem,
    recv_sem,
    tp_send,
    tp_recv,
):
    me = lax.axis_index("kv")
    core = lax.axis_index("tp")
    rows, width = residual_ref.shape
    model = 2 * width
    total = n_kv * rows
    packed = rows * GROUPS
    part = rows // HALVES
    part_total = n_kv * part
    part_packed = part * GROUPS
    planes = n_kv // PLANE
    half_planes = planes // 2
    depth_at, spot = me // PLANE, lax.rem(me, PLANE)
    spot_x, spot_y = lax.rem(spot, 2), spot // 2
    slot = lax.rem(me, GROUPS)
    owner_core = me // GROUPS
    holder = core == HOLDER
    owns = jnp.logical_and(holder, owner_core == HOLDER)
    f32, bf16 = jnp.float32, jnp.bfloat16

    def flipped(flip):
        return 2 * lax.rem(spot_y + flip // 2, 2) + lax.rem(spot_x + flip % 2, 2)

    def others():
        for flip in FLIPS:
            for step in range(planes - 1, -1, -1):
                plane = 2 * lax.rem(depth_at // 2 + step // 2, 2) + lax.rem(depth_at + step, 2)
                if step or flip:
                    yield plane * PLANE + flipped(flip)

    def load(index, source, target):
        return pltpu.make_async_copy(source, target, load_sem.at[index])

    loads = [
        load(0, forget_hbm, own_weights.at[0]),
        load(1, value_hbm, own_weights.at[1]),
        load(2, query_hbm, own_weights.at[2]),
        load(3, outgate_hbm, own_weights.at[3]),
        load(4, gate_pre_hbm, gate_pre),
        load(5, up_pre_hbm, up_pre),
        load(6, down_pre_hbm, down_pre),
        load(7, state_hbm, state),
        load(8, out_hbm.at[:, pl.ds(0, width)], out_weight.at[0]),
        load(12, out_hbm.at[:, pl.ds(width, width)], out_weight.at[1]),
        load(9, gate_post_hbm, gate_post),
        load(10, up_post_hbm, up_post),
        load(11, down_post_hbm, down_post),
    ]
    for copy in loads:
        copy.start()

    def spread_rows(target, values):
        for group in range(GROUPS):
            target[pl.ds(group, values.shape[0], stride=GROUPS), :] = values[:, lanes(group)]

    residual = residual_ref[...].astype(f32)
    spread_rows(stream_rows, residual)
    packed_parts = [
        slice(half * part_packed, (half + 1) * part_packed) for half in range(HALVES)
    ]
    for half in range(HALVES):
        gather_a[half, me] = stream_rows[packed_parts[half], :].astype(bf16)

    barrier = pltpu.get_barrier_semaphore()
    for peer in others():
        pl.semaphore_signal(
            barrier, inc=1, device_id={"kv": peer}, device_id_type=pl.DeviceIdType.MESH
        )
    pl.semaphore_signal(
        barrier, inc=1, device_id={"tp": 1 - core}, device_id_type=pl.DeviceIdType.MESH
    )
    pl.semaphore_wait(barrier, n_kv)

    def remote(exchange, source, target, **device):
        return pltpu.make_async_remote_copy(
            src_ref=source,
            dst_ref=target,
            send_sem=send_sem.at[exchange],
            recv_sem=recv_sem.at[exchange],
            device_id=device,
            device_id_type=pl.DeviceIdType.MESH,
        )

    def all_of(exchange, ref):
        return remote(exchange, ref, ref, tp=1 - core)

    def tp_copy(index, source, target):
        return pltpu.make_async_remote_copy(
            src_ref=source,
            dst_ref=target,
            send_sem=tp_send.at[index],
            recv_sem=tp_recv.at[index],
            device_id={"tp": 1 - core},
            device_id_type=pl.DeviceIdType.MESH,
        )

    def gate_up(which, half, gathered, wide, gain_ref, gate, up):
        wide[half] = gathered[half].astype(f32).reshape(part_total * GROUPS, LANES)
        square_lanes = jnp.zeros((part_total, LANES), f32)
        for group in range(GROUPS):
            piece = wide[half, pl.ds(group, part_total, stride=GROUPS), :]
            square_lanes += piece * piece
            scaled_rows[half, :, lanes(group)] = (piece * gain_ref[:, lanes(group)]).astype(bf16)
        scaled = scaled_rows[half]
        squares = jnp.sum(square_lanes, axis=1, keepdims=True)
        squares_out[which, half] = jnp.broadcast_to(squares, squares_out.shape[2:])
        first = 6 * which + 3 * half
        copies = [
            tp_copy(first, squares_out.at[which, half], squares_in.at[which, half]),
            tp_copy(first + 1, gate_up_out.at[which, half, 0], gate_up_in.at[which, half, 0]),
            tp_copy(first + 2, gate_up_out.at[which, half, 1], gate_up_in.at[which, half, 1]),
        ]
        gate_part = jnp.dot(scaled, gate[...], preferred_element_type=f32)
        gate_up_out[which, half, 0] = gate_part.astype(bf16)
        copies[0].start()
        copies[1].start()
        up_part = jnp.dot(scaled, up[...], preferred_element_type=f32)
        gate_up_out[which, half, 1] = up_part.astype(bf16)
        copies[2].start()
        return squares, gate_part, up_part, copies

    def down_sum(which, half, parts, down):
        squares, gate_part, up_part, copies = parts
        for copy in copies:
            copy.wait_recv()
        inverse = lax.rsqrt((squares + squares_in[which, half][:, 0:1]) / model + EPSILON)
        gate_sum = (gate_part + gate_up_in[which, half, 0].astype(f32)) * inverse
        up_sum = (up_part + gate_up_in[which, half, 1].astype(f32)) * inverse
        hidden = (gate_sum / (1.0 + jnp.exp(-gate_sum)) * up_sum).astype(bf16)
        return jnp.dot(hidden, down[...], preferred_element_type=f32)

    def gather_start(exchange, gathered):
        for half in range(HALVES):
            block = gathered.at[half, me]
            for peer in others():
                remote(exchange + half, block, block, kv=peer).start()

    def turn(target, source):
        for group in range(GROUPS):
            target[lanes(group), :] = source[:, lanes(group)].T

    def but_one(ref, half):
        return ref.at[half, pl.ds(0, n_kv - 1)]

    gather_start(GATHER_A, gather_a)
    for copy in loads[0:4]:
        copy.wait()
    def send_weights(source, target_core, flips):
        for flip, low, high in flips:
            peer_spot = flipped(flip)
            span = pl.ds(low, high - low)
            remote(
                WEIGHTS + target_core,
                source.at[peer_spot, span],
                plane_weights.at[spot, span],
                kv=depth_at * PLANE + peer_spot,
                tp=target_core,
            ).start()

    @pl.when(holder)
    def _():
        for flip in FLIPS[1:3] + FLIPS[0:1]:
            block = flipped(flip)
            remote(RELAY, own_weights.at[block], relayed.at[block], tp=1 - core).start()

    @pl.when(jnp.logical_not(holder))
    def _():
        send_weights(own_weights, 1 - HOLDER, WEIGHTS_EARLY)
        all_of(RELAY, relayed.at[pl.ds(0, PLANE - 1)]).wait_recv()
        send_weights(relayed, HOLDER, WEIGHTS_EARLY)

    plane_weights[spot] = own_weights[spot]
    mixed_rows[packed:, :] = jnp.zeros((mixed_rows.shape[0] - packed, LANES), f32)
    for copy in loads[4:7]:
        copy.wait()
    turn(gate_pre_t, gate_pre)
    turn(up_pre_t, up_pre)
    parts_a = []
    for half in range(HALVES):
        all_of(GATHER_A + half, but_one(gather_a, half)).wait_recv()
        parts_a.append(
            gate_up(0, half, gather_a, wide_a, gain_pre_ref, gate_pre_t, up_pre_t)
        )
    shared_copies = [
        tp_copy(COLUMNS + half, shared_out.at[half], shared_in.at[half]) for half in range(HALVES)
    ]

    @pl.when(owner_core == core)
    def _():
        for half in range(HALVES):
            shared_out[half] = wide_a[half, pl.ds(slot, part_total, stride=GROUPS), :].astype(bf16)

        @pl.when(jnp.logical_not(holder))
        def _():
            for copy in shared_copies:
                copy.start()

    for half in range(HALVES):
        branch_a = down_sum(0, half, parts_a[half], down_pre)
        for group in range(GROUPS):
            columns_out[half, group] = branch_a[:, lanes(group)].astype(bf16)
        for flip in FLIPS:
            for step in range(half_planes - 1, -1, -1):
                plane = core * half_planes + lax.rem(depth_at + step, half_planes)
                peer = plane * PLANE + flipped(flip)
                copy = remote(
                    SCATTER_A + half,
                    columns_out.at[half, lax.rem(peer, GROUPS)],
                    columns_landed.at[half, me],
                    kv=peer,
                    tp=HOLDER,
                )
                if step or flip:
                    copy.start()
                else:
                    pl.when(jnp.logical_not(owns))(copy.start)

    @pl.when(jnp.logical_not(holder))
    def _():
        send_weights(own_weights, 1 - HOLDER, WEIGHTS_LATE)
        send_weights(relayed, HOLDER, WEIGHTS_LATE)

    @pl.when(holder)
    def _():
        for half in range(HALVES):

            @pl.when(owns)
            def _():
                columns_landed[half, me] = columns_out[half, slot]
                shared_in[half] = shared_out[half]
                all_of(SCATTER_A + half, but_one(columns_landed, half)).wait_recv()

            @pl.when(jnp.logical_not(owns))
            def _():
                shared_copies[half].wait_recv()
                all_of(SCATTER_A + half, columns_landed.at[half]).wait_recv()

            branch = jnp.sum(columns_landed[half].astype(f32), axis=0)
            stream = (shared_in[half].astype(f32) + 0.5 * branch).astype(bf16).astype(f32)
            columns_in[half, spot] = (stream * gain_mix_ref[me]).astype(bf16)
            block = columns_in.at[half, spot]
            for flip in FLIPS:
                peer = depth_at * PLANE + flipped(flip)
                remote(SHARE + half, block, block, kv=peer, tp=1 - core).start()
                if flip:
                    remote(SHARE + half, block, block, kv=peer, tp=core).start()
            for owner in range(n_kv):
                rows_out[owner, half * part : (half + 1) * part, :] = stream[
                    owner * part : (owner + 1) * part, :
                ]
        for peer in others():
            remote(ROWS, rows_out.at[peer], rows_in.at[slot], kv=peer, tp=owner_core).start()

        @pl.when(owns)
        def _():
            rows_in[slot] = rows_out[me]

        @pl.when(jnp.logical_not(owns))
        def _():
            remote(ROWS, rows_out.at[me], rows_in.at[slot], tp=1 - core).start()

    for half in range(HALVES):

        @pl.when(holder)
        def _():
            all_of(SHARE + half, columns_in.at[half, pl.ds(0, PLANE - 1)]).wait_recv()

        @pl.when(jnp.logical_not(holder))
        def _():
            all_of(SHARE + half, columns_in.at[half]).wait_recv()

        if half == 0:
            all_of(WEIGHTS + core, plane_weights.at[pl.ds(0, PLANE - 1)]).wait_recv()
        columns = jnp.concatenate([columns_in[half, place] for place in range(PLANE)], axis=1)
        product = jnp.dot(
            columns,
            plane_weights[...].reshape(PLANE * LANES, width),
            preferred_element_type=f32,
        )
        spread_rows(spread.at[half], product)
        proj_out[half] = spread[half].astype(bf16).reshape(n_kv, part_packed, LANES)
        for peer in others():
            remote(PROJECT + half, proj_out.at[half, peer], proj_in.at[half, me], kv=peer).start()
        proj_in[half, me] = proj_out[half, me]

    @pl.when(owns)
    def _():
        all_of(ROWS, rows_in.at[pl.ds(0, GROUPS - 1)]).wait_recv()

    @pl.when(jnp.logical_not(owns))
    def _():
        all_of(ROWS, rows_in).wait_recv()

    for group in range(GROUPS):
        stream_rows[pl.ds(group, rows, stride=GROUPS), :] = rows_in[group]
    stream = stream_rows[...].reshape(rows, GROUPS, LANES)
    row_squares = jnp.sum(stream * stream, axis=1)
    row_squares_out[...] = row_squares
    square_copy = tp_copy(SQUARES, row_squares_out, row_squares_in)
    square_copy.start()
    loads[7].wait()
    for row in range(rows):
        for head in range(GROUPS):
            state_half[row // 2, head * LANES : (head + 1) * LANES, lanes(row % 2)] = state[
                row, head
            ].astype(bf16)
    for copy in loads[10:12]:
        copy.wait()
    turn(gate_post_t, gate_post)
    turn(up_post_t, up_post)
    square_copy.wait_recv()
    squares = jnp.sum(row_squares + row_squares_in[...], axis=1, keepdims=True)
    inverse = lax.rsqrt(squares / model + EPSILON)
    for row in range(rows):
        inverse_rows[row * GROUPS : (row + 1) * GROUPS, :] = jnp.broadcast_to(
            inverse[row : row + 1, :], (GROUPS, LANES)
        )
    loads[8].wait()
    loads[9].wait()
    for half in range(HALVES):
        all_of(PROJECT + half, but_one(proj_in, half)).wait_recv()

    def projected(index):
        sums = []
        for half in range(HALVES):
            terms = [proj_in[half, plane * PLANE + index].astype(f32) for plane in range(planes)]
            sums.append(sum(terms[1:], terms[0]))
        return jnp.concatenate(sums, axis=0) * inverse_rows[...]

    floor_rate = jnp.concatenate([lower_ref[...]] * rows, axis=0)
    forget_pre = projected(0)
    keep = floor_rate + (1.0 - floor_rate) / (1.0 + jnp.exp(-forget_pre))
    inject = (1.0 - floor_rate) / (1.0 + jnp.exp(forget_pre))
    query_pre = projected(2)
    query = query_pre / (1.0 + jnp.exp(-query_pre))
    value = projected(1)
    value_rows[...] = value
    weighted = query * keep
    direct = jnp.sum(query * inject, axis=1, keepdims=True) * value
    head_index = lax.broadcasted_iota(jnp.int32, (GROUPS, LANES), 0)
    read = []
    for pair in range(rows // 2):
        diagonal = []
        for row in (2 * pair, 2 * pair + 1):
            heads = weighted[row * GROUPS : (row + 1) * GROUPS, :]
            diagonal.append(
                jnp.concatenate(
                    [jnp.where(head_index == head, heads, 0.0) for head in range(GROUPS)], axis=1
                )
            )
        both = jnp.dot(
            jnp.concatenate(diagonal, axis=0).astype(bf16),
            state_half[pair],
            preferred_element_type=f32,
        )
        read.append(both[0:GROUPS, lanes(0)])
        read.append(both[GROUPS : 2 * GROUPS, lanes(1)])
    readout = jnp.concatenate(read, axis=0) + direct
    outgate_pre = projected(3)
    outgate = outgate_pre / (1.0 + jnp.exp(-outgate_pre))
    scale = lax.rsqrt(jnp.mean(readout * readout, axis=1, keepdims=True) + EPSILON)
    head_gain = jnp.concatenate([head_gain_ref[...]] * rows, axis=0)
    mixed_rows[0:packed, :] = readout * scale * head_gain * outgate
    mixed_heads = jnp.concatenate(
        [mixed_rows[pl.ds(head, GROUPS, stride=GROUPS), :] for head in range(GROUPS)], axis=1
    ).astype(bf16)
    away = jnp.dot(mixed_heads, out_weight[1 - core], preferred_element_type=f32)
    spread_rows(mixed_out, away[0:rows])
    mixed_copy = tp_copy(MIXED, mixed_out, mixed_in)
    mixed_copy.start()
    home = jnp.dot(mixed_heads, out_weight[core], preferred_element_type=f32)
    spread_rows(mixed_own, home[0:rows])
    for row in range(rows):
        span = slice(row * GROUPS, (row + 1) * GROUPS)
        keep_t[row] = keep[span].T
        inject_t[row] = inject[span].T
    mixed_copy.wait_recv()
    stream_b = (stream_rows[...] + (mixed_own[...] + mixed_in[...])).astype(bf16)
    for half in range(HALVES):
        gather_b[half, me] = stream_b[packed_parts[half], :]
    gather_start(GATHER_B, gather_b)

    def update(row, carry):
        keep_columns = keep_t[row]
        inject_columns = inject_t[row]
        for head in range(GROUPS):
            column = slice(head, head + 1)
            values = value_rows[pl.ds(row * GROUPS + head, 1), :]
            next_ref[row, head] = (
                keep_columns[:, column] * state[row, head] + inject_columns[:, column] * values
            )
        return carry

    lax.fori_loop(0, rows, update, 0)
    loads[12].wait()
    parts_b = []
    for half in range(HALVES):
        all_of(GATHER_B + half, but_one(gather_b, half)).wait_recv()
        parts_b.append(
            gate_up(1, half, gather_b, wide_b, gain_post_ref, gate_post_t, up_post_t)
        )
    for half in range(HALVES):
        branch_b = down_sum(1, half, parts_b[half], down_post)
        spread_rows(spread.at[half], branch_b)
        partial_b[half] = spread[half].astype(bf16).reshape(n_kv, part_packed, LANES)
        for peer in others():
            remote(
                SCATTER_B + half, partial_b.at[half, peer], landed_b.at[half, me], kv=peer
            ).start()
        landed_b[half, me] = partial_b[half, me]
    for copy in parts_a[0][3] + parts_a[1][3] + parts_b[0][3] + parts_b[1][3]:
        copy.wait_send()
    square_copy.wait_send()
    mixed_copy.wait_send()
    for half in range(HALVES):
        all_of(GATHER_A + half, but_one(gather_a, half)).wait_send()
        all_of(PROJECT + half, but_one(proj_out, half)).wait_send()
        all_of(GATHER_B + half, but_one(gather_b, half)).wait_send()

    @pl.when(jnp.logical_not(holder))
    def _():
        for target_core in range(2):
            all_of(WEIGHTS + target_core, plane_weights.at[pl.ds(0, PLANE - 1)]).wait_send()

    @pl.when(holder)
    def _():
        all_of(RELAY, relayed.at[pl.ds(0, PLANE - 1)]).wait_send()
        for half in range(HALVES):
            all_of(SHARE + half, columns_landed.at[half, pl.ds(0, 2 * PLANE - 1)]).wait_send()

    @pl.when(owns)
    def _():
        for half in range(HALVES):
            all_of(SCATTER_A + half, columns_out.at[half, pl.ds(0, GROUPS - 1)]).wait_send()
        all_of(ROWS, rows_out.at[pl.ds(0, n_kv - 1)]).wait_send()

    @pl.when(jnp.logical_not(owns))
    def _():
        for half in range(HALVES):
            all_of(SCATTER_A + half, columns_out.at[half]).wait_send()

        @pl.when(holder)
        def _():
            all_of(ROWS, rows_out).wait_send()

    @pl.when(jnp.logical_and(owner_core == core, jnp.logical_not(holder)))
    def _():
        for copy in shared_copies:
            copy.wait_send()

    for half in range(HALVES):
        all_of(SCATTER_B + half, but_one(landed_b, half)).wait_recv()
        branch = jnp.sum(landed_b[half].astype(f32), axis=0)
        mixed_rows[packed_parts[half], :] = gather_b[half, me].astype(f32) + 0.5 * branch
    for group in range(GROUPS):
        layer_ref[:, lanes(group)] = mixed_rows[pl.ds(group, rows, stride=GROUPS), :].astype(bf16)
    for half in range(HALVES):
        all_of(SCATTER_B + half, but_one(partial_b, half)).wait_send()


def store_results(layer_in, state_in, layer_out, state_out, sem):
    copies = [pltpu.make_async_copy(layer_in, layer_out, sem.at[0])]
    for row in range(state_in.shape[0]):
        copies.append(pltpu.make_async_copy(state_in.at[row], state_out.at[row], sem.at[1 + row]))
    for copy in copies:
        copy.start()
    for copy in copies:
        copy.wait()


def fused_shards(
    n_kv,
    residual_in,
    gain_pre,
    gate_pre,
    up_pre,
    down_pre,
    gain_mix,
    query_weight,
    forget_weight,
    value_weight,
    outgate_weight,
    lower_bound,
    head_gain,
    out_weight,
    gain_post,
    gate_post,
    up_post,
    down_post,
    memory_state,
):
    rows, width = residual_in.shape
    hidden = gate_pre.shape[1]
    total = n_kv * rows
    packed = rows * GROUPS
    f32, bf16 = jnp.float32, jnp.bfloat16
    vmem = pl.BlockSpec(memory_space=pltpu.VMEM)
    hbm = pl.BlockSpec(memory_space=pltpu.HBM)
    like = lambda array: pltpu.VMEM(array.shape, array.dtype)
    part_total = total // HALVES
    blocks = lambda: pltpu.VMEM((HALVES, n_kv, packed // HALVES, LANES), bf16)
    halves = lambda *shape: pltpu.VMEM((HALVES,) + shape, bf16)
    outs = (
        jax.ShapeDtypeStruct(residual_in.shape, residual_in.dtype),
        jax.ShapeDtypeStruct(memory_state.shape, memory_state.dtype),
    )
    layer, state = pl.pallas_call(
        functools.partial(fused_layer, n_kv),
        out_shape=tuple(pltpu.VMEM(out.shape, out.dtype) for out in outs),
        in_specs=[vmem] * 6 + [hbm] * 12,
        out_specs=(vmem, vmem),
        scratch_shapes=[
            pltpu.VMEM((hidden, width), bf16),
            pltpu.VMEM((hidden, width), bf16),
            like(down_pre),
            pltpu.VMEM((PLANE,) + query_weight.shape, bf16),
            pltpu.VMEM((PLANE,) + query_weight.shape, bf16),
            pltpu.VMEM((PLANE,) + query_weight.shape, bf16),
            pltpu.VMEM((2, width, width), bf16),
            pltpu.VMEM((hidden, width), bf16),
            pltpu.VMEM((hidden, width), bf16),
            like(down_post),
            pltpu.VMEM((width, hidden), bf16),
            pltpu.VMEM((width, hidden), bf16),
            pltpu.VMEM((width, hidden), bf16),
            pltpu.VMEM((width, hidden), bf16),
            like(memory_state),
            pltpu.VMEM((rows // 2, width, 2 * LANES), bf16),
            blocks(),
            blocks(),
            pltpu.VMEM((HALVES, part_total * GROUPS, LANES), f32),
            pltpu.VMEM((HALVES, part_total * GROUPS, LANES), f32),
            pltpu.VMEM((HALVES, part_total * GROUPS, LANES), f32),
            halves(part_total, width),
            halves(GROUPS, part_total, LANES),
            halves(n_kv, part_total, LANES),
            halves(PLANE, part_total, LANES),
            halves(part_total, LANES),
            halves(part_total, LANES),
            pltpu.VMEM((n_kv, rows, LANES), f32),
            pltpu.VMEM((GROUPS, rows, LANES), f32),
            pltpu.VMEM((packed, LANES), f32),
            blocks(),
            blocks(),
            pltpu.VMEM((packed, LANES), f32),
            pltpu.VMEM((rows, LANES, GROUPS), f32),
            pltpu.VMEM((rows, LANES, GROUPS), f32),
            pltpu.VMEM((packed, LANES), f32),
            pltpu.VMEM((GROUPS * GROUPS, LANES), f32),
            pltpu.VMEM((packed, LANES), f32),
            pltpu.VMEM((packed, LANES), f32),
            pltpu.VMEM((packed, LANES), f32),
            blocks(),
            blocks(),
            pltpu.VMEM((2, HALVES, 2, part_total, hidden), bf16),
            pltpu.VMEM((2, HALVES, 2, part_total, hidden), bf16),
            pltpu.VMEM((2, HALVES, part_total, LANES), f32),
            pltpu.VMEM((2, HALVES, part_total, LANES), f32),
            pltpu.VMEM((rows, LANES), f32),
            pltpu.VMEM((rows, LANES), f32),
            pltpu.SemaphoreType.DMA((13,)),
            pltpu.SemaphoreType.DMA((EXCHANGES,)),
            pltpu.SemaphoreType.DMA((EXCHANGES,)),
            pltpu.SemaphoreType.DMA((TP_EXCHANGES,)),
            pltpu.SemaphoreType.DMA((TP_EXCHANGES,)),
        ],
        compiler_params=pltpu.CompilerParams(
            collective_id=0, has_side_effects=True, vmem_limit_bytes=56 * 1024 * 1024
        ),
    )(
        residual_in,
        gain_pre.reshape(1, width),
        gain_mix.reshape(n_kv, 1, LANES),
        lower_bound.reshape(GROUPS, LANES),
        head_gain.reshape(GROUPS, LANES),
        gain_post.reshape(1, width),
        gate_pre.T,
        up_pre.T,
        down_pre,
        query_weight,
        forget_weight,
        value_weight,
        outgate_weight,
        out_weight,
        gate_post.T,
        up_post.T,
        down_post,
        memory_state,
    )
    return pl.pallas_call(
        store_results,
        out_shape=outs,
        in_specs=[vmem, vmem],
        out_specs=(hbm, hbm),
        scratch_shapes=[pltpu.SemaphoreType.DMA((1 + rows,))],
        compiler_params=pltpu.CompilerParams(vmem_limit_bytes=8 * 1024 * 1024),
    )(layer, state)


def solution(mesh):
    n_kv, n_tp = mesh.shape["kv"], mesh.shape["tp"]
    fits = n_tp == 2 and n_kv * LANES == D and n_kv // n_tp == GROUPS
    body = functools.partial(fused_shards, n_kv) if fits else shards
    in_specs = (
        P("kv", "tp"),
        P("tp"),
        P("tp", "kv"),
        P("tp", "kv"),
        P("kv", "tp"),
        P(),
        P("kv", "tp"),
        P("kv", "tp"),
        P("kv", "tp"),
        P("kv", "tp"),
        P("tp"),
        P("tp"),
        P("tp", None),
        P("tp"),
        P("tp", "kv"),
        P("tp", "kv"),
        P("kv", "tp"),
        P("kv", "tp", None, None),
    )
    out_specs = (P("kv", "tp"), P("kv", "tp", None, None))
    return jax.shard_map(body, mesh=mesh, in_specs=in_specs, out_specs=out_specs, check_vma=False)
```

```python
import functools

import jax
import jax.numpy as jnp
from jax import lax
from jax.experimental import pallas as pl
from jax.experimental.pallas import tpu as pltpu
from jax.sharding import PartitionSpec as P

D = 2048
HEAD_DIM = 128


EPSILON = 1e-06


def channel_mixer(row_block, gain_vec, gate_weight, up_weight, down_weight):
    gathered = lax.all_gather(row_block, "kv", axis=0, tiled=True)
    widened = gathered.astype(jnp.float32)
    part_squares = jnp.sum(widened * widened, axis=1)
    scaled = (widened * gain_vec).astype(jnp.bfloat16)
    gate_part = jnp.dot(scaled, gate_weight, preferred_element_type=jnp.float32)
    up_part = jnp.dot(scaled, up_weight, preferred_element_type=jnp.float32)
    gate_share, up_share, square_share = (
        lax.psum_scatter(
            gate_part.astype(jnp.bfloat16), "tp", scatter_dimension=0, tiled=True
        ).astype(jnp.float32),
        lax.psum_scatter(
            up_part.astype(jnp.bfloat16), "tp", scatter_dimension=0, tiled=True
        ).astype(jnp.float32),
        lax.psum_scatter(
            part_squares.astype(jnp.bfloat16), "tp", scatter_dimension=0, tiled=True
        ).astype(jnp.float32),
    )
    share_inverse = lax.rsqrt(square_share / D + EPSILON)[:, None]
    hidden_share = (jax.nn.silu(gate_share * share_inverse) * (up_share * share_inverse)).astype(
        jnp.bfloat16
    )
    hidden = lax.all_gather(hidden_share, "tp", axis=0, tiled=True)
    return lax.psum_scatter(
        jnp.dot(hidden, down_weight, preferred_element_type=jnp.float32),
        "kv",
        scatter_dimension=0,
        tiled=True,
    )


def token_mixer(
    stream_a,
    gain_mix,
    query_weight,
    forget_weight,
    value_weight,
    outgate_weight,
    lower_bound,
    head_gain,
    out_weight,
    memory_state,
):
    full_rows = lax.all_gather(stream_a, "tp", axis=1, tiled=True)
    widened = full_rows.astype(jnp.float32)
    inverse = lax.rsqrt(jnp.mean(widened * widened, axis=1, keepdims=True) + EPSILON)
    scaled = (widened * gain_mix).astype(jnp.bfloat16)
    weights = (query_weight, forget_weight, value_weight, outgate_weight)
    blocks = lax.all_to_all(scaled, "kv", split_axis=1, concat_axis=0, tiled=True)
    joined = jnp.concatenate(weights, axis=1)
    projected = lax.psum_scatter(
        jnp.dot(blocks, joined, preferred_element_type=jnp.float32),
        "kv",
        scatter_dimension=0,
        tiled=True,
    )
    projected = projected * inverse
    seq_rows = scaled.shape[0]
    local_heads = query_weight.shape[1] // HEAD_DIM
    reshaped = projected.reshape(seq_rows, 4, local_heads, HEAD_DIM)
    query_pre = reshaped[:, 0]
    forget_pre = reshaped[:, 1]
    value_pre = reshaped[:, 2]
    outgate_pre = reshaped[:, 3]
    floor_rate = lower_bound.reshape(local_heads, HEAD_DIM)
    log_keep = jnp.logaddexp(
        jnp.log(floor_rate), jnp.log1p(-floor_rate) + jax.nn.log_sigmoid(forget_pre)
    )
    inject = (1.0 - floor_rate) * jax.nn.sigmoid(-forget_pre)
    next_state = (
        jnp.exp(log_keep)[..., None] * memory_state + inject[..., None] * value_pre[:, :, None, :]
    )
    readout = jnp.einsum(
        "bhk,bhkv->bhv", jax.nn.silu(query_pre), next_state, precision=lax.Precision.HIGHEST
    )
    normed = (
        readout
        * lax.rsqrt(jnp.mean(readout * readout, axis=2, keepdims=True) + EPSILON)
        * head_gain.reshape(local_heads, HEAD_DIM)
    )
    mixed_heads = (
        (normed * jax.nn.silu(outgate_pre))
        .reshape(seq_rows, local_heads * HEAD_DIM)
        .astype(jnp.bfloat16)
    )
    partial_out = jnp.dot(mixed_heads, out_weight, preferred_element_type=jnp.float32)
    mixed = lax.psum_scatter(
        partial_out.astype(jnp.bfloat16), "tp", scatter_dimension=1, tiled=True
    ).astype(jnp.float32)
    return (mixed, next_state)


def shards(
    residual_in,
    gain_pre,
    gate_pre,
    up_pre,
    down_pre,
    gain_mix,
    query_weight,
    forget_weight,
    value_weight,
    outgate_weight,
    lower_bound,
    head_gain,
    out_weight,
    gain_post,
    gate_post,
    up_post,
    down_post,
    memory_state,
):
    branch_a = channel_mixer(residual_in, gain_pre, gate_pre, up_pre, down_pre)
    stream_a = (residual_in.astype(jnp.float32) + 0.5 * branch_a).astype(jnp.bfloat16)
    mixed, next_state = token_mixer(
        stream_a,
        gain_mix,
        query_weight,
        forget_weight,
        value_weight,
        outgate_weight,
        lower_bound,
        head_gain,
        out_weight,
        memory_state,
    )
    stream_b = (stream_a.astype(jnp.float32) + mixed).astype(jnp.bfloat16)
    branch_b = channel_mixer(stream_b, gain_post, gate_post, up_post, down_post)
    layer_out = (stream_b.astype(jnp.float32) + 0.5 * branch_b).astype(jnp.bfloat16)
    return (layer_out, next_state)


LANES = 128
GROUPS = 8
PLANE = 4
HALVES = 2
GATHER_A, SCATTER_A, SHARE, PROJECT, GATHER_B, SCATTER_B, WEIGHTS, ROWS = range(0, 16, HALVES)
EXCHANGES = 17
RELAY = 16
SQUARES, MIXED, COLUMNS = 12, 13, 14
TP_EXCHANGES = 16
HOLDER = 1
EARLY_ROWS = LANES // 4
WEIGHTS_EARLY = ((3, 0, LANES), (1, 0, EARLY_ROWS), (2, 0, EARLY_ROWS))
WEIGHTS_LATE = ((1, EARLY_ROWS, LANES), (2, EARLY_ROWS, LANES))
FLIPS = (3, 1, 2, 0)


def lanes(group):
    return slice(group * LANES, (group + 1) * LANES)


def fused_layer(
    n_kv,
    residual_ref,
    gain_pre_ref,
    gain_mix_ref,
    lower_ref,
    head_gain_ref,
    gain_post_ref,
    gate_pre_hbm,
    up_pre_hbm,
    down_pre_hbm,
    query_hbm,
    forget_hbm,
    value_hbm,
    outgate_hbm,
    out_hbm,
    gate_post_hbm,
    up_post_hbm,
    down_post_hbm,
    state_hbm,
    layer_ref,
    next_ref,
    gate_pre,
    up_pre,
    down_pre,
    own_weights,
    plane_weights,
    relayed,
    out_weight,
    gate_post,
    up_post,
    down_post,
    gate_pre_t,
    up_pre_t,
    gate_post_t,
    up_post_t,
    state,
    state_half,
    gather_a,
    gather_b,
    wide_a,
    wide_b,
    spread,
    scaled_rows,
    columns_out,
    columns_landed,
    columns_in,
    shared_out,
    shared_in,
    rows_out,
    rows_in,
    stream_rows,
    proj_out,
    proj_in,
    inverse_rows,
    keep_t,
    inject_t,
    value_rows,
    mixed_rows,
    mixed_out,
    mixed_own,
    mixed_in,
    partial_b,
    landed_b,
    gate_up_out,
    gate_up_in,
    squares_out,
    squares_in,
    row_squares_out,
    row_squares_in,
    load_sem,
    send_sem,
    recv_sem,
    tp_send,
    tp_recv,
):
    me = lax.axis_index("kv")
    core = lax.axis_index("tp")
    rows, width = residual_ref.shape
    model = 2 * width
    total = n_kv * rows
    packed = rows * GROUPS
    part = rows // HALVES
    part_total = n_kv * part
    part_packed = part * GROUPS
    planes = n_kv // PLANE
    half_planes = planes // 2
    depth_at, spot = me // PLANE, lax.rem(me, PLANE)
    spot_x, spot_y = lax.rem(spot, 2), spot // 2
    slot = lax.rem(me, GROUPS)
    owner_core = me // GROUPS
    holder = core == HOLDER
    owns = jnp.logical_and(holder, owner_core == HOLDER)
    f32, bf16 = jnp.float32, jnp.bfloat16

    def flipped(flip):
        return 2 * lax.rem(spot_y + flip // 2, 2) + lax.rem(spot_x + flip % 2, 2)

    def others():
        for flip in FLIPS:
            for step in range(planes - 1, -1, -1):
                plane = 2 * lax.rem(depth_at // 2 + step // 2, 2) + lax.rem(depth_at + step, 2)
                if step or flip:
                    yield plane * PLANE + flipped(flip)

    def load(index, source, target):
        return pltpu.make_async_copy(source, target, load_sem.at[index])

    loads = [
        load(0, forget_hbm, own_weights.at[0]),
        load(1, value_hbm, own_weights.at[1]),
        load(2, query_hbm, own_weights.at[2]),
        load(3, outgate_hbm, own_weights.at[3]),
        load(4, gate_pre_hbm, gate_pre),
        load(5, up_pre_hbm, up_pre),
        load(6, down_pre_hbm, down_pre),
        load(7, state_hbm, state),
        load(8, out_hbm.at[:, pl.ds(0, width)], out_weight.at[0]),
        load(12, out_hbm.at[:, pl.ds(width, width)], out_weight.at[1]),
        load(9, gate_post_hbm, gate_post),
        load(10, up_post_hbm, up_post),
        load(11, down_post_hbm, down_post),
    ]
    for copy in loads:
        copy.start()

    def spread_rows(target, values):
        for group in range(GROUPS):
            target[pl.ds(group, values.shape[0], stride=GROUPS), :] = values[:, lanes(group)]

    residual = residual_ref[...].astype(f32)
    spread_rows(stream_rows, residual)
    packed_parts = [
        slice(half * part_packed, (half + 1) * part_packed) for half in range(HALVES)
    ]
    for half in range(HALVES):
        gather_a[half, me] = stream_rows[packed_parts[half], :].astype(bf16)

    barrier = pltpu.get_barrier_semaphore()
    for peer in others():
        pl.semaphore_signal(
            barrier, inc=1, device_id={"kv": peer}, device_id_type=pl.DeviceIdType.MESH
        )
    pl.semaphore_signal(
        barrier, inc=1, device_id={"tp": 1 - core}, device_id_type=pl.DeviceIdType.MESH
    )
    pl.semaphore_wait(barrier, n_kv)

    def remote(exchange, source, target, **device):
        return pltpu.make_async_remote_copy(
            src_ref=source,
            dst_ref=target,
            send_sem=send_sem.at[exchange],
            recv_sem=recv_sem.at[exchange],
            device_id=device,
            device_id_type=pl.DeviceIdType.MESH,
        )

    def all_of(exchange, ref):
        return remote(exchange, ref, ref, tp=1 - core)

    def tp_copy(index, source, target):
        return pltpu.make_async_remote_copy(
            src_ref=source,
            dst_ref=target,
            send_sem=tp_send.at[index],
            recv_sem=tp_recv.at[index],
            device_id={"tp": 1 - core},
            device_id_type=pl.DeviceIdType.MESH,
        )

    def gate_up(which, half, gathered, wide, gain_ref, gate, up):
        wide[half] = gathered[half].astype(f32).reshape(part_total * GROUPS, LANES)
        square_lanes = jnp.zeros((part_total, LANES), f32)
        for group in range(GROUPS):
            piece = wide[half, pl.ds(group, part_total, stride=GROUPS), :]
            square_lanes += piece * piece
            scaled_rows[half, :, lanes(group)] = (piece * gain_ref[:, lanes(group)]).astype(bf16)
        scaled = scaled_rows[half]
        squares = jnp.sum(square_lanes, axis=1, keepdims=True)
        squares_out[which, half] = jnp.broadcast_to(squares, squares_out.shape[2:])
        first = 6 * which + 3 * half
        copies = [
            tp_copy(first, squares_out.at[which, half], squares_in.at[which, half]),
            tp_copy(first + 1, gate_up_out.at[which, half, 0], gate_up_in.at[which, half, 0]),
            tp_copy(first + 2, gate_up_out.at[which, half, 1], gate_up_in.at[which, half, 1]),
        ]
        gate_part = jnp.dot(scaled, gate[...], preferred_element_type=f32)
        gate_up_out[which, half, 0] = gate_part.astype(bf16)
        copies[0].start()
        copies[1].start()
        up_part = jnp.dot(scaled, up[...], preferred_element_type=f32)
        gate_up_out[which, half, 1] = up_part.astype(bf16)
        copies[2].start()
        return squares, gate_part, up_part, copies

    def down_sum(which, half, parts, down):
        squares, gate_part, up_part, copies = parts
        for copy in copies:
            copy.wait_recv()
        inverse = lax.rsqrt((squares + squares_in[which, half][:, 0:1]) / model + EPSILON)
        gate_sum = (gate_part + gate_up_in[which, half, 0].astype(f32)) * inverse
        up_sum = (up_part + gate_up_in[which, half, 1].astype(f32)) * inverse
        hidden = (gate_sum / (1.0 + jnp.exp(-gate_sum)) * up_sum).astype(bf16)
        return jnp.dot(hidden, down[...], preferred_element_type=f32)

    def gather_start(exchange, gathered):
        for half in range(HALVES):
            block = gathered.at[half, me]
            for peer in others():
                remote(exchange + half, block, block, kv=peer).start()

    def turn(target, source):
        for group in range(GROUPS):
            target[lanes(group), :] = source[:, lanes(group)].T

    def but_one(ref, half):
        return ref.at[half, pl.ds(0, n_kv - 1)]

    gather_start(GATHER_A, gather_a)
    for copy in loads[0:4]:
        copy.wait()
    def send_weights(source, target_core, flips):
        for flip, low, high in flips:
            peer_spot = flipped(flip)
            span = pl.ds(low, high - low)
            remote(
                WEIGHTS + target_core,
                source.at[peer_spot, span],
                plane_weights.at[spot, span],
                kv=depth_at * PLANE + peer_spot,
                tp=target_core,
            ).start()

    @pl.when(holder)
    def _():
        for flip in FLIPS[1:3] + FLIPS[0:1]:
            block = flipped(flip)
            remote(RELAY, own_weights.at[block], relayed.at[block], tp=1 - core).start()

    @pl.when(jnp.logical_not(holder))
    def _():
        send_weights(own_weights, 1 - HOLDER, WEIGHTS_EARLY)
        all_of(RELAY, relayed.at[pl.ds(0, PLANE - 1)]).wait_recv()
        send_weights(relayed, HOLDER, WEIGHTS_EARLY)

    plane_weights[spot] = own_weights[spot]
    mixed_rows[packed:, :] = jnp.zeros((mixed_rows.shape[0] - packed, LANES), f32)
    for copy in loads[4:7]:
        copy.wait()
    turn(gate_pre_t, gate_pre)
    turn(up_pre_t, up_pre)
    parts_a = []
    for half in range(HALVES):
        all_of(GATHER_A + half, but_one(gather_a, half)).wait_recv()
        parts_a.append(
            gate_up(0, half, gather_a, wide_a, gain_pre_ref, gate_pre_t, up_pre_t)
        )
    shared_copies = [
        tp_copy(COLUMNS + half, shared_out.at[half], shared_in.at[half]) for half in range(HALVES)
    ]

    @pl.when(owner_core == core)
    def _():
        for half in range(HALVES):
            shared_out[half] = wide_a[half, pl.ds(slot, part_total, stride=GROUPS), :].astype(bf16)

        @pl.when(jnp.logical_not(holder))
        def _():
            for copy in shared_copies:
                copy.start()

    for half in range(HALVES):
        branch_a = down_sum(0, half, parts_a[half], down_pre)
        for group in range(GROUPS):
            columns_out[half, group] = branch_a[:, lanes(group)].astype(bf16)
        for flip in FLIPS:
            for step in range(half_planes - 1, -1, -1):
                plane = core * half_planes + lax.rem(depth_at + step, half_planes)
                peer = plane * PLANE + flipped(flip)
                copy = remote(
                    SCATTER_A + half,
                    columns_out.at[half, lax.rem(peer, GROUPS)],
                    columns_landed.at[half, me],
                    kv=peer,
                    tp=HOLDER,
                )
                if step or flip:
                    copy.start()
                else:
                    pl.when(jnp.logical_not(owns))(copy.start)

    @pl.when(jnp.logical_not(holder))
    def _():
        send_weights(own_weights, 1 - HOLDER, WEIGHTS_LATE)
        send_weights(relayed, HOLDER, WEIGHTS_LATE)

    @pl.when(holder)
    def _():
        for half in range(HALVES):

            @pl.when(owns)
            def _():
                columns_landed[half, me] = columns_out[half, slot]
                shared_in[half] = shared_out[half]
                all_of(SCATTER_A + half, but_one(columns_landed, half)).wait_recv()

            @pl.when(jnp.logical_not(owns))
            def _():
                shared_copies[half].wait_recv()
                all_of(SCATTER_A + half, columns_landed.at[half]).wait_recv()

            branch = jnp.sum(columns_landed[half].astype(f32), axis=0)
            stream = (shared_in[half].astype(f32) + 0.5 * branch).astype(bf16).astype(f32)
            columns_in[half, spot] = (stream * gain_mix_ref[me]).astype(bf16)
            block = columns_in.at[half, spot]
            for flip in FLIPS:
                peer = depth_at * PLANE + flipped(flip)
                remote(SHARE + half, block, block, kv=peer, tp=1 - core).start()
                if flip:
                    remote(SHARE + half, block, block, kv=peer, tp=core).start()
            for owner in range(n_kv):
                rows_out[owner, half * part : (half + 1) * part, :] = stream[
                    owner * part : (owner + 1) * part, :
                ]
        for peer in others():
            remote(ROWS, rows_out.at[peer], rows_in.at[slot], kv=peer, tp=owner_core).start()

        @pl.when(owns)
        def _():
            rows_in[slot] = rows_out[me]

        @pl.when(jnp.logical_not(owns))
        def _():
            remote(ROWS, rows_out.at[me], rows_in.at[slot], tp=1 - core).start()

    for half in range(HALVES):

        @pl.when(holder)
        def _():
            all_of(SHARE + half, columns_in.at[half, pl.ds(0, PLANE - 1)]).wait_recv()

        @pl.when(jnp.logical_not(holder))
        def _():
            all_of(SHARE + half, columns_in.at[half]).wait_recv()

        if half == 0:
            all_of(WEIGHTS + core, plane_weights.at[pl.ds(0, PLANE - 1)]).wait_recv()
        columns = jnp.concatenate([columns_in[half, place] for place in range(PLANE)], axis=1)
        product = jnp.dot(
            columns,
            plane_weights[...].reshape(PLANE * LANES, width),
            preferred_element_type=f32,
        )
        spread_rows(spread.at[half], product)
        proj_out[half] = spread[half].astype(bf16).reshape(n_kv, part_packed, LANES)
        for peer in others():
            remote(PROJECT + half, proj_out.at[half, peer], proj_in.at[half, me], kv=peer).start()
        proj_in[half, me] = proj_out[half, me]

    @pl.when(owns)
    def _():
        all_of(ROWS, rows_in.at[pl.ds(0, GROUPS - 1)]).wait_recv()

    @pl.when(jnp.logical_not(owns))
    def _():
        all_of(ROWS, rows_in).wait_recv()

    for group in range(GROUPS):
        stream_rows[pl.ds(group, rows, stride=GROUPS), :] = rows_in[group]
    stream = stream_rows[...].reshape(rows, GROUPS, LANES)
    row_squares = jnp.sum(stream * stream, axis=1)
    row_squares_out[...] = row_squares
    square_copy = tp_copy(SQUARES, row_squares_out, row_squares_in)
    square_copy.start()
    loads[7].wait()
    for row in range(rows):
        for head in range(GROUPS):
            state_half[row // 2, head * LANES : (head + 1) * LANES, lanes(row % 2)] = state[
                row, head
            ].astype(bf16)
    for copy in loads[10:12]:
        copy.wait()
    turn(gate_post_t, gate_post)
    turn(up_post_t, up_post)
    square_copy.wait_recv()
    squares = jnp.sum(row_squares + row_squares_in[...], axis=1, keepdims=True)
    inverse = lax.rsqrt(squares / model + EPSILON)
    for row in range(rows):
        inverse_rows[row * GROUPS : (row + 1) * GROUPS, :] = jnp.broadcast_to(
            inverse[row : row + 1, :], (GROUPS, LANES)
        )
    loads[8].wait()
    loads[9].wait()
    floor_rate = jnp.concatenate([lower_ref[...]] * part, axis=0)
    head_index = lax.broadcasted_iota(jnp.int32, (GROUPS, LANES), 0)
    keeps, injects, weights, directs, outgates, read = [], [], [], [], [], []

    def diagonal(row):
        span = slice(row % part * GROUPS, (row % part + 1) * GROUPS)
        heads = weights[row // part][span]
        return jnp.concatenate(
            [jnp.where(head_index == head, heads, 0.0) for head in range(GROUPS)], axis=1
        )

    def read_pairs(ready):
        while len(read) + 1 < ready:
            row = len(read)
            both = jnp.dot(
                jnp.concatenate([diagonal(row), diagonal(row + 1)], axis=0).astype(bf16),
                state_half[row // 2],
                preferred_element_type=f32,
            )
            read.append(both[0:GROUPS, lanes(0)])
            read.append(both[GROUPS : 2 * GROUPS, lanes(1)])

    for half in range(HALVES):
        all_of(PROJECT + half, but_one(proj_in, half)).wait_recv()

        def projected(index):
            terms = [proj_in[half, plane * PLANE + index].astype(f32) for plane in range(planes)]
            return sum(terms[1:], terms[0]) * inverse_rows[packed_parts[half], :]

        forget_pre = projected(0)
        keeps.append(floor_rate + (1.0 - floor_rate) / (1.0 + jnp.exp(-forget_pre)))
        injects.append((1.0 - floor_rate) / (1.0 + jnp.exp(forget_pre)))
        query_pre = projected(2)
        query = query_pre / (1.0 + jnp.exp(-query_pre))
        value = projected(1)
        value_rows[packed_parts[half], :] = value
        weights.append(query * keeps[half])
        directs.append(jnp.sum(query * injects[half], axis=1, keepdims=True) * value)
        outgate_pre = projected(3)
        outgates.append(outgate_pre / (1.0 + jnp.exp(-outgate_pre)))
        read_pairs((half + 1) * part)
    keep = jnp.concatenate(keeps, axis=0)
    inject = jnp.concatenate(injects, axis=0)
    outgate = jnp.concatenate(outgates, axis=0)
    readout = jnp.concatenate(read, axis=0) + jnp.concatenate(directs, axis=0)
    scale = lax.rsqrt(jnp.mean(readout * readout, axis=1, keepdims=True) + EPSILON)
    head_gain = jnp.concatenate([head_gain_ref[...]] * rows, axis=0)
    mixed_rows[0:packed, :] = readout * scale * head_gain * outgate
    mixed_heads = jnp.concatenate(
        [mixed_rows[pl.ds(head, GROUPS, stride=GROUPS), :] for head in range(GROUPS)], axis=1
    ).astype(bf16)
    away = jnp.dot(mixed_heads, out_weight[1 - core], preferred_element_type=f32)
    spread_rows(mixed_out, away[0:rows])
    mixed_copy = tp_copy(MIXED, mixed_out, mixed_in)
    mixed_copy.start()
    home = jnp.dot(mixed_heads, out_weight[core], preferred_element_type=f32)
    spread_rows(mixed_own, home[0:rows])
    for row in range(rows):
        span = slice(row * GROUPS, (row + 1) * GROUPS)
        keep_t[row] = keep[span].T
        inject_t[row] = inject[span].T
    mixed_copy.wait_recv()
    stream_b = (stream_rows[...] + (mixed_own[...] + mixed_in[...])).astype(bf16)
    for half in range(HALVES):
        gather_b[half, me] = stream_b[packed_parts[half], :]
    gather_start(GATHER_B, gather_b)

    def update(row, carry):
        keep_columns = keep_t[row]
        inject_columns = inject_t[row]
        for head in range(GROUPS):
            column = slice(head, head + 1)
            values = value_rows[pl.ds(row * GROUPS + head, 1), :]
            next_ref[row, head] = (
                keep_columns[:, column] * state[row, head] + inject_columns[:, column] * values
            )
        return carry

    lax.fori_loop(0, rows, update, 0)
    loads[12].wait()
    parts_b = []
    for half in range(HALVES):
        all_of(GATHER_B + half, but_one(gather_b, half)).wait_recv()
        parts_b.append(
            gate_up(1, half, gather_b, wide_b, gain_post_ref, gate_post_t, up_post_t)
        )
    for half in range(HALVES):
        branch_b = down_sum(1, half, parts_b[half], down_post)
        spread_rows(spread.at[half], branch_b)
        partial_b[half] = spread[half].astype(bf16).reshape(n_kv, part_packed, LANES)
        for peer in others():
            remote(
                SCATTER_B + half, partial_b.at[half, peer], landed_b.at[half, me], kv=peer
            ).start()
        landed_b[half, me] = partial_b[half, me]
    for copy in parts_a[0][3] + parts_a[1][3] + parts_b[0][3] + parts_b[1][3]:
        copy.wait_send()
    square_copy.wait_send()
    mixed_copy.wait_send()
    for half in range(HALVES):
        all_of(GATHER_A + half, but_one(gather_a, half)).wait_send()
        all_of(PROJECT + half, but_one(proj_out, half)).wait_send()
        all_of(GATHER_B + half, but_one(gather_b, half)).wait_send()

    @pl.when(jnp.logical_not(holder))
    def _():
        for target_core in range(2):
            all_of(WEIGHTS + target_core, plane_weights.at[pl.ds(0, PLANE - 1)]).wait_send()

    @pl.when(holder)
    def _():
        all_of(RELAY, relayed.at[pl.ds(0, PLANE - 1)]).wait_send()
        for half in range(HALVES):
            all_of(SHARE + half, columns_landed.at[half, pl.ds(0, 2 * PLANE - 1)]).wait_send()

    @pl.when(owns)
    def _():
        for half in range(HALVES):
            all_of(SCATTER_A + half, columns_out.at[half, pl.ds(0, GROUPS - 1)]).wait_send()
        all_of(ROWS, rows_out.at[pl.ds(0, n_kv - 1)]).wait_send()

    @pl.when(jnp.logical_not(owns))
    def _():
        for half in range(HALVES):
            all_of(SCATTER_A + half, columns_out.at[half]).wait_send()

        @pl.when(holder)
        def _():
            all_of(ROWS, rows_out).wait_send()

    @pl.when(jnp.logical_and(owner_core == core, jnp.logical_not(holder)))
    def _():
        for copy in shared_copies:
            copy.wait_send()

    for half in range(HALVES):
        all_of(SCATTER_B + half, but_one(landed_b, half)).wait_recv()
        branch = jnp.sum(landed_b[half].astype(f32), axis=0)
        mixed_rows[packed_parts[half], :] = gather_b[half, me].astype(f32) + 0.5 * branch
    for group in range(GROUPS):
        layer_ref[:, lanes(group)] = mixed_rows[pl.ds(group, rows, stride=GROUPS), :].astype(bf16)
    for half in range(HALVES):
        all_of(SCATTER_B + half, but_one(partial_b, half)).wait_send()


def store_results(layer_in, state_in, layer_out, state_out, sem):
    copies = [pltpu.make_async_copy(layer_in, layer_out, sem.at[0])]
    for row in range(state_in.shape[0]):
        copies.append(pltpu.make_async_copy(state_in.at[row], state_out.at[row], sem.at[1 + row]))
    for copy in copies:
        copy.start()
    for copy in copies:
        copy.wait()


def fused_shards(
    n_kv,
    residual_in,
    gain_pre,
    gate_pre,
    up_pre,
    down_pre,
    gain_mix,
    query_weight,
    forget_weight,
    value_weight,
    outgate_weight,
    lower_bound,
    head_gain,
    out_weight,
    gain_post,
    gate_post,
    up_post,
    down_post,
    memory_state,
):
    rows, width = residual_in.shape
    hidden = gate_pre.shape[1]
    total = n_kv * rows
    packed = rows * GROUPS
    f32, bf16 = jnp.float32, jnp.bfloat16
    vmem = pl.BlockSpec(memory_space=pltpu.VMEM)
    hbm = pl.BlockSpec(memory_space=pltpu.HBM)
    like = lambda array: pltpu.VMEM(array.shape, array.dtype)
    part_total = total // HALVES
    blocks = lambda: pltpu.VMEM((HALVES, n_kv, packed // HALVES, LANES), bf16)
    halves = lambda *shape: pltpu.VMEM((HALVES,) + shape, bf16)
    outs = (
        jax.ShapeDtypeStruct(residual_in.shape, residual_in.dtype),
        jax.ShapeDtypeStruct(memory_state.shape, memory_state.dtype),
    )
    layer, state = pl.pallas_call(
        functools.partial(fused_layer, n_kv),
        out_shape=tuple(pltpu.VMEM(out.shape, out.dtype) for out in outs),
        in_specs=[vmem] * 6 + [hbm] * 12,
        out_specs=(vmem, vmem),
        scratch_shapes=[
            pltpu.VMEM((hidden, width), bf16),
            pltpu.VMEM((hidden, width), bf16),
            like(down_pre),
            pltpu.VMEM((PLANE,) + query_weight.shape, bf16),
            pltpu.VMEM((PLANE,) + query_weight.shape, bf16),
            pltpu.VMEM((PLANE,) + query_weight.shape, bf16),
            pltpu.VMEM((2, width, width), bf16),
            pltpu.VMEM((hidden, width), bf16),
            pltpu.VMEM((hidden, width), bf16),
            like(down_post),
            pltpu.VMEM((width, hidden), bf16),
            pltpu.VMEM((width, hidden), bf16),
            pltpu.VMEM((width, hidden), bf16),
            pltpu.VMEM((width, hidden), bf16),
            like(memory_state),
            pltpu.VMEM((rows // 2, width, 2 * LANES), bf16),
            blocks(),
            blocks(),
            pltpu.VMEM((HALVES, part_total * GROUPS, LANES), f32),
            pltpu.VMEM((HALVES, part_total * GROUPS, LANES), f32),
            pltpu.VMEM((HALVES, part_total * GROUPS, LANES), f32),
            halves(part_total, width),
            halves(GROUPS, part_total, LANES),
            halves(n_kv, part_total, LANES),
            halves(PLANE, part_total, LANES),
            halves(part_total, LANES),
            halves(part_total, LANES),
            pltpu.VMEM((n_kv, rows, LANES), f32),
            pltpu.VMEM((GROUPS, rows, LANES), f32),
            pltpu.VMEM((packed, LANES), f32),
            blocks(),
            blocks(),
            pltpu.VMEM((packed, LANES), f32),
            pltpu.VMEM((rows, LANES, GROUPS), f32),
            pltpu.VMEM((rows, LANES, GROUPS), f32),
            pltpu.VMEM((packed, LANES), f32),
            pltpu.VMEM((GROUPS * GROUPS, LANES), f32),
            pltpu.VMEM((packed, LANES), f32),
            pltpu.VMEM((packed, LANES), f32),
            pltpu.VMEM((packed, LANES), f32),
            blocks(),
            blocks(),
            pltpu.VMEM((2, HALVES, 2, part_total, hidden), bf16),
            pltpu.VMEM((2, HALVES, 2, part_total, hidden), bf16),
            pltpu.VMEM((2, HALVES, part_total, LANES), f32),
            pltpu.VMEM((2, HALVES, part_total, LANES), f32),
            pltpu.VMEM((rows, LANES), f32),
            pltpu.VMEM((rows, LANES), f32),
            pltpu.SemaphoreType.DMA((13,)),
            pltpu.SemaphoreType.DMA((EXCHANGES,)),
            pltpu.SemaphoreType.DMA((EXCHANGES,)),
            pltpu.SemaphoreType.DMA((TP_EXCHANGES,)),
            pltpu.SemaphoreType.DMA((TP_EXCHANGES,)),
        ],
        compiler_params=pltpu.CompilerParams(
            collective_id=0, has_side_effects=True, vmem_limit_bytes=56 * 1024 * 1024
        ),
    )(
        residual_in,
        gain_pre.reshape(1, width),
        gain_mix.reshape(n_kv, 1, LANES),
        lower_bound.reshape(GROUPS, LANES),
        head_gain.reshape(GROUPS, LANES),
        gain_post.reshape(1, width),
        gate_pre.T,
        up_pre.T,
        down_pre,
        query_weight,
        forget_weight,
        value_weight,
        outgate_weight,
        out_weight,
        gate_post.T,
        up_post.T,
        down_post,
        memory_state,
    )
    return pl.pallas_call(
        store_results,
        out_shape=outs,
        in_specs=[vmem, vmem],
        out_specs=(hbm, hbm),
        scratch_shapes=[pltpu.SemaphoreType.DMA((1 + rows,))],
        compiler_params=pltpu.CompilerParams(vmem_limit_bytes=8 * 1024 * 1024),
    )(layer, state)


def solution(mesh):
    n_kv, n_tp = mesh.shape["kv"], mesh.shape["tp"]
    fits = n_tp == 2 and n_kv * LANES == D and n_kv // n_tp == GROUPS
    body = functools.partial(fused_shards, n_kv) if fits else shards
    in_specs = (
        P("kv", "tp"),
        P("tp"),
        P("tp", "kv"),
        P("tp", "kv"),
        P("kv", "tp"),
        P(),
        P("kv", "tp"),
        P("kv", "tp"),
        P("kv", "tp"),
        P("kv", "tp"),
        P("tp"),
        P("tp"),
        P("tp", None),
        P("tp"),
        P("tp", "kv"),
        P("tp", "kv"),
        P("kv", "tp"),
        P("kv", "tp", None, None),
    )
    out_specs = (P("kv", "tp"), P("kv", "tp", None, None))
    return jax.shard_map(body, mesh=mesh, in_specs=in_specs, out_specs=out_specs, check_vma=False)
```
